512 devices in a mesh: rep: 2 (over z_hi), fs: 32 (over z_lo, y), tp: 8 (over x, core).
Axes of the slice: x: 4, y: 8, z: 8 (z_hi: 2, z_lo: 4; z = z_hi * 4 + z_lo), core: 2. Of those that a mesh axis runs over, the one named last changes fastest.
Arguments:
- states: bfloat16 [24576, 2048], P(('rep', 'fs'), 'tp'), may hold values from -6 to 6
- mix_gain: float32 [2048], replicated, may hold values from 0.1 to 1.9
- w_value: bfloat16 [2048, 2048], P('fs', 'tp'), may hold values from -1 to 1
- w_gate: bfloat16 [2048, 2048], P('fs', 'tp'), may hold values from -0.125 to 0.125
- conv_kernel: float32 [31, 2048], replicated, may hold values from -1 to 1
- chan_gain: float32 [2048], replicated, may hold values from 0.1 to 1.9
- w_mix_out: bfloat16 [2048, 2048], P('fs', 'tp'), may hold values from -0.125 to 0.125
- mlp_gain: float32 [2048], replicated, may hold values from 0.1 to 1.9
- w_up: bfloat16 [2048, 6144], P('fs', 'tp'), may hold values from -0.125 to 0.125
- w_down_t: bfloat16 [2048, 6144], P('fs', 'tp'), may hold values from -0.078125 to 0.078125
Outputs:
- layer_out: bfloat16 [24576, 2048], P(('rep', 'fs'), 'tp')
The draws below stay inside these ranges and needn't reach their ends.
All inputs are finite; a program needn't handle non-finite values.
Results may differ from the reference program's by a relative error of at most 0.017.
Values may be sent and summed in bfloat16 or wider, within the bound.
A program may use at most 64 MiB of HBM per device.

```python
import jax
import jax.numpy as jnp
from jax import lax

D = 2048
FF = 6144
KWIDTH = 31
LENGTH = 128
SEQS = 3
ROWS = 384
TOKENS = 24576
N_TP = 8


def draw_w_value(key, part):
    first_key, second_key = jax.random.split(jax.random.fold_in(key, 17))
    column = jnp.arange(D, dtype=jnp.float32)
    ramp = 10.0 ** (column / D)
    base = jnp.clip(jax.random.normal(first_key, (D, D), jnp.float32), -6.0, 6.0)
    jitter = jax.random.uniform(second_key, (D,), jnp.float32, 0.7, 1.3)
    scale = ramp * jitter / (3.0 * jnp.sqrt(jnp.float32(D)))
    return jnp.clip(base * scale[None, :], -1.0, 1.0).astype(jnp.bfloat16)


def shard_levels(own_key, shape, cuts, low, high):
    loudness, own = 1.0, jax.random.fold_in(own_key, 6)
    for position, blocks in cuts:
        heights = jnp.exp(jax.random.uniform(jax.random.fold_in(own, position), (blocks,), jnp.float32, low / len(cuts), high / len(cuts)))
        loudness = loudness * jnp.repeat(heights, shape[position] // blocks).reshape([-1 if axis == position else 1 for axis in range(len(shape))])
    return loudness


def normal_values(key, shape, deviation, most, cuts=(), kind=jnp.bfloat16):
    values = deviation * jax.random.normal(key, shape, jnp.float32)
    if cuts:
        values = values * shard_levels(key, shape, cuts, -0.22, 0.18)
    return jnp.clip(values, -most, most).astype(kind)


def setup_inputs(seed: int = 0) -> dict:
    arg_keys = jax.random.split(jax.random.key(seed), 11)
    return {
        "states": normal_values(arg_keys[0], (TOKENS, D), 1.0, 6.0, ((0, 64), (1, 8))),
        "mix_gain": jnp.clip(1.0 + 0.18 * jax.random.normal(arg_keys[1], (D,), jnp.float32), 0.1, 1.9),
        "w_value": draw_w_value(jax.random.fold_in(arg_keys[10], 71), 0),
        "w_gate": normal_values(arg_keys[3], (D, D), D ** -0.5, 0.125, ((0, 32), (1, 8))),
        "conv_kernel": normal_values(arg_keys[4], (KWIDTH, D), KWIDTH ** -0.5, 1.0, (), jnp.float32),
        "chan_gain": jnp.clip(1.0 + 0.18 * jax.random.normal(arg_keys[5], (D,), jnp.float32), 0.1, 1.9),
        "w_mix_out": normal_values(arg_keys[6], (D, D), D ** -0.5, 0.125, ((0, 32), (1, 8))),
        "mlp_gain": jnp.clip(1.0 + 0.18 * jax.random.normal(arg_keys[7], (D,), jnp.float32), 0.1, 1.9),
        "w_up": normal_values(arg_keys[8], (D, FF), D ** -0.5, 0.125, ((0, 32), (1, 8))),
        "w_down_t": normal_values(arg_keys[9], (D, FF), FF ** -0.5, 0.078125, ((0, 32), (1, 8))),
    }


EPS = 1e-06

def rms_norm(rows, gain):
    values = rows.astype(jnp.float32)
    scaled = values * lax.rsqrt(lax.optimization_barrier(jnp.mean(values * values, axis=-1, keepdims=True)) + EPS)
    return (scaled * gain).astype(jnp.bfloat16)

def causal_filter(gated, conv_kernel):
    width = gated.shape[1]
    blocks = gated.reshape(SEQS, LENGTH, width)
    padded = jnp.pad(blocks, ((0, 0), (KWIDTH - 1, 0), (0, 0)))
    total = jnp.zeros_like(blocks)
    for tap in range(KWIDTH):
        total = total + conv_kernel[tap][None, None, :] * padded[:, tap:tap + LENGTH, :]
    return total.reshape(SEQS * LENGTH, width)

def project_out(activated, weight_t):
    block = activated.shape[1] // N_TP
    total = jnp.zeros((activated.shape[0], weight_t.shape[0]), jnp.float32)
    for index in range(N_TP):
        piece = lax.dot_general(activated[:, index * block:(index + 1) * block], weight_t[:, index * block:(index + 1) * block], (((1,), (1,)), ((), ())), preferred_element_type=jnp.float32)
        total = total + piece.astype(jnp.bfloat16).astype(jnp.float32)
    return total

def one_group(rows, mix_gain, w_value, w_gate, conv_kernel, chan_gain, w_mix_out, mlp_gain, w_up, w_down_t):
    normed = rms_norm(rows, mix_gain)
    value = jnp.dot(normed, w_value, preferred_element_type=jnp.float32)
    gate = jnp.dot(normed, w_gate, preferred_element_type=jnp.float32)
    gated = value * jax.nn.sigmoid(gate)
    filtered = causal_filter(gated, conv_kernel)
    mean_rows = lax.optimization_barrier(jnp.mean(filtered, axis=-1, keepdims=True))
    variance = lax.optimization_barrier(jnp.mean(filtered * filtered, axis=-1, keepdims=True)) - mean_rows * mean_rows
    activated = jax.nn.silu((filtered - mean_rows) * lax.rsqrt(variance + EPS) * chan_gain).astype(jnp.bfloat16)
    middle = (rows.astype(jnp.float32) + project_out(activated, w_mix_out)).astype(jnp.bfloat16)
    normed_mid = rms_norm(middle, mlp_gain)
    upward = jnp.dot(normed_mid, w_up, preferred_element_type=jnp.float32)
    hidden = jnp.square(jnp.maximum(upward, 0.0)).astype(jnp.bfloat16)
    return (middle.astype(jnp.float32) + project_out(hidden, w_down_t)).astype(jnp.bfloat16)

def reference(states, mix_gain, w_value, w_gate, conv_kernel, chan_gain, w_mix_out, mlp_gain, w_up, w_down_t):
    groups = states.reshape(states.shape[0] // ROWS, ROWS, states.shape[1])

    def apply(rows):
        return one_group(rows, mix_gain, w_value, w_gate, conv_kernel, chan_gain, w_mix_out, mlp_gain, w_up, w_down_t)
    return lax.map(apply, groups).reshape(states.shape)
```

```python
import functools

import jax
import jax.numpy as jnp
from jax import lax
from jax.experimental import pallas as pl
from jax.experimental.pallas import tpu as pltpu
from jax.sharding import PartitionSpec as P

D = 2048
KWIDTH = 31
LENGTH = 128
SEQS = 3
EPS = 1e-06
F32 = jnp.float32
BF16 = jnp.bfloat16

TENSORS = {"vg": (512, 32), "mx": (256, 32), "up": (768, 48), "dn": (768, 32)}
RANK = {"vg": 0, "mx": 1, "up": 2, "dn": 3}
GROUPS = ((0, 1), (6, 8), (1, 3), (3, 6))
FORWARD_SEQS = (0, 2)

RATE = 46600.0
SIBLING_RATE = 300000.0
HOP = 2.2
SIBLING_HOP = 1.0
WINDOW = 4.0


class Plan:
    def __init__(self, send_sems, recv_sems):
        self.copies, self.tasks = {}, {}
        self.send_sems, self.recv_sems = send_sems, recv_sems

    def copy(self, name, src, dst, device, link, needs=(), rank=0):
        index = len(self.copies)
        size = 2 if src.dtype == BF16 else 4
        for extent in src.shape:
            size *= extent
        descriptor = pltpu.make_async_remote_copy(
            src_ref=src,
            dst_ref=dst,
            send_sem=self.send_sems.at[index],
            recv_sem=self.recv_sems.at[index],
            device_id=device,
            device_id_type=pl.DeviceIdType.MESH,
        )
        self.copies[name] = (descriptor, link, size, frozenset(needs), rank)

    def task(self, name, fn, needs, time, rank):
        self.tasks[name] = (fn, frozenset(needs), time, rank)

    def emit(self):
        now, done, free = 0.0, set(), {}
        arrives, waiting = {}, dict(self.copies)
        tasks = dict(self.tasks)
        while waiting or arrives or tasks:
            for name in sorted(waiting, key=lambda n: waiting[n][4]):
                descriptor, link, size, needs, _ = waiting[name]
                if needs <= done and free.get(link, 0.0) - now < WINDOW:
                    near = link == "d"
                    took = size / (SIBLING_RATE if near else RATE)
                    free[link] = max(free.get(link, 0.0), now) + took
                    arrives[name] = free[link] + (SIBLING_HOP if near else HOP)
                    descriptor.start()
                    del waiting[name]
            here = [n for n in arrives if arrives[n] <= now]
            if here:
                first = min(here, key=lambda n: arrives[n])
                self.copies[first][0].wait_recv()
                del arrives[first]
                done.add(first)
                now += 0.02
                continue
            ready = [n for n in tasks if tasks[n][1] <= done]
            if ready:
                best = min(ready, key=lambda n: tasks[n][3])
                fn, _, time, _ = tasks.pop(best)
                fn()
                done.add(best)
                now += time
                continue
            later = list(arrives.values())
            for name in waiting:
                _, link, _, needs, _ = waiting[name]
                if needs <= done:
                    later.append(free[link] - WINDOW + 0.001)
            now = max(now, min(later)) + 1e-6
        for descriptor, *_ in self.copies.values():
            descriptor.wait_send()
        return now


def kernel(
    states, w_value, w_gate, w_mix, w_up, w_down, conv, chan, mix_gain, mlp_gain, out,
    vg, mx, up, dn, full, taps, chan_own, padded, filtered, stats, stats_in, activated, hidden,
    to_sibling, from_sibling, kept, sent, relay_part, relayed, arrived,
    local_sems, send_sems, recv_sems,
):
    rep, fs, tp = lax.axis_index("rep"), lax.axis_index("fs"), lax.axis_index("tp")
    y, z_lo = lax.rem(fs, 8), fs // 8
    z = rep * 4 + z_lo
    x, core = tp // 2, lax.rem(tp, 2)
    step8, step4 = 1 + 6 * core, 1 + 2 * core

    def y_to(hops):
        return {"fs": z_lo * 8 + lax.rem(y + hops * step8, 8)}

    def z_to(hops):
        there = lax.rem(z + hops * step8, 8)
        return {"rep": there // 4, "fs": lax.rem(there, 4) * 8 + y}

    def x_to(hops):
        return {"tp": lax.rem(x + hops * step4, 4) * 2 + core}

    y_ahead, y_back, z_ahead, z_back = y_to(1), y_to(7), z_to(1), z_to(7)
    x_ahead, x_back = x_to(1), x_to(3)
    sibling = {"tp": tp + 1 - 2 * core}

    own = pl.ds(pl.multiple_of(tp * 256, 256), 256)
    loads = [
        (states, full.at[0, 0, 0]),
        (w_value, vg.at[0, 0, :, 0:256]),
        (w_gate, vg.at[0, 0, :, 256:512]),
        (w_mix, mx.at[0, 0]),
        (w_up, up.at[0, 0]),
        (w_down, dn.at[0, 0]),
        (conv.at[:, own], taps),
        (chan.at[:, own], chan_own),
    ]
    loads = [pltpu.make_async_copy(a, b, local_sems.at[i]) for i, (a, b) in enumerate(loads)]
    for load in loads:
        load.start()

    barrier = pltpu.get_barrier_semaphore()
    peers = [y_ahead, y_back, z_ahead, z_back]
    peers += [{"tp": lax.rem(tp + j, 8)} for j in range(1, 8)]
    for peer in peers:
        pl.semaphore_signal(
            barrier, inc=1, device_id=peer, device_id_type=pl.DeviceIdType.MESH
        )
    for tile in range(2):
        for s in range(SEQS):
            padded[tile, s, 0:32, :] = jnp.zeros((32, 128), F32)
    for load in loads:
        load.wait()
    pl.semaphore_wait(barrier, len(peers))

    plan = Plan(send_sems, recv_sems)

    complete = {}
    for name, ref in (("vg", vg), ("mx", mx), ("up", up), ("dn", dn)):
        cut, rank = TENSORS[name][1], RANK[name] * 10
        before = set(plan.copies)
        low, high = pl.ds(0, cut), pl.ds(cut, 64 - cut)
        for d in range(1, 5):
            needs = [f"{name}yF{d - 1}"] if d > 1 else []
            plan.copy(
                f"{name}yF{d}", ref.at[(9 - d) % 8, 0, low], ref.at[8 - d, 0, low], y_ahead, "yF", needs, rank + 1
            )
        for d in range(1, 4):
            needs = [f"{name}yR{d - 1}"] if d > 1 else []
            plan.copy(
                f"{name}yR{d}", ref.at[d - 1, 0, low], ref.at[d, 0, low], y_back, "yR", needs, rank + 1
            )
        group_needs = (
            [],
            [f"{name}yF1", f"{name}yF2"],
            [f"{name}yR1", f"{name}yR2"],
            [f"{name}yR3", f"{name}yF3", f"{name}yF4"],
        )
        for g, (lo, hi) in enumerate(GROUPS):
            rows = pl.ds(lo, hi - lo)
            plan.copy(
                f"{name}zF{g}", ref.at[rows, 0, low], ref.at[rows, 3, low], z_ahead, "zF", group_needs[g], rank + 2
            )
            plan.copy(
                f"{name}zR{g}", ref.at[rows, 0, low], ref.at[rows, 1, low], z_back, "zR", group_needs[g], rank + 2
            )
            if g in (0, 3):
                plan.copy(
                    f"{name}zX{g}", ref.at[rows, 3, low], ref.at[rows, 2, low], z_ahead, "zF", [f"{name}zF{g}"], rank + 2
                )
            else:
                plan.copy(
                    f"{name}zX{g}", ref.at[rows, 1, low], ref.at[rows, 2, low], z_back, "zR", [f"{name}zR{g}"], rank + 2
                )
        plan.copy(f"{name}bF", ref.at[0, 0, high], ref.at[0, 3, high], z_ahead, "zF", [], rank)
        plan.copy(f"{name}bR", ref.at[0, 0, high], ref.at[0, 1, high], z_back, "zR", [], rank)
        plan.copy(
            f"{name}bX", ref.at[0, 3, high], ref.at[0, 2, high], z_ahead, "zF", [f"{name}bF"], rank
        )
        first = [f"{name}bF", f"{name}bR", f"{name}bX"]
        for d in range(1, 5):
            needs = [f"{name}cF{d - 1}"] if d > 1 else first
            plan.copy(
                f"{name}cF{d}", ref.at[(9 - d) % 8, :, high], ref.at[8 - d, :, high], y_ahead, "yF", needs, rank
            )
        for d in range(1, 4):
            needs = [f"{name}cR{d - 1}"] if d > 1 else first
            plan.copy(
                f"{name}cR{d}", ref.at[d - 1, :, high], ref.at[d, :, high], y_back, "yR", needs, rank
            )
        complete[name] = set(plan.copies) - before

    def shards(ref, block):
        at_z = lax.rem((block // 2 + 4 - z_lo) * step4, 4)
        pieces = []
        for i in range(4):
            at_y = lax.rem((lax.rem(block, 2) * 4 + i + 8 - y) * step8, 8)
            pieces.append(ref[at_y, at_z])
        return jnp.concatenate(pieces, axis=0)

    gathered = {}
    for p in range(2):
        for s in range(SEQS):
            rows = full.at[p]
            needs = [f"mid{s}"] if p else []
            name = f"g{p}{s}"
            mine = rows.at[0, 0, s]
            plan.copy(f"{name}F", mine, rows.at[0, 3, s], x_ahead, "xF", needs, 2 + s)
            plan.copy(f"{name}R", mine, rows.at[0, 1, s], x_back, "xR", needs, 2 + s)
            plan.copy(f"{name}S0", mine, rows.at[1, 0, s], sibling, "d", needs, 2 + s)
            if s in FORWARD_SEQS:
                plan.copy(f"{name}X", rows.at[0, 3, s], rows.at[0, 2, s], x_ahead, "xF", [f"{name}F"], 1 + s)
            else:
                plan.copy(f"{name}X", rows.at[0, 1, s], rows.at[0, 2, s], x_back, "xR", [f"{name}R"], 1 + s)
            plan.copy(f"{name}S3", rows.at[0, 3, s], rows.at[1, 1, s], sibling, "d", [f"{name}F"], 2 + s)
            plan.copy(f"{name}S1", rows.at[0, 1, s], rows.at[1, 3, s], sibling, "d", [f"{name}R"], 2 + s)
            plan.copy(f"{name}S2", rows.at[0, 2, s], rows.at[1, 2, s], sibling, "d", [f"{name}X"], 2 + s)
            gathered[p, s] = [name + k for k in ("F", "R", "S0", "X", "S3", "S1", "S2")]

    def normalised(p, s, gain):
        squares = jnp.zeros((LENGTH, 256), F32)
        for side in range(2):
            for at in range(4):
                values = full[p, side, at, s].astype(F32)
                squares = squares + values * values
        scale = lax.rsqrt(jnp.sum(squares, axis=-1, keepdims=True) / D + EPS)
        blocks = []
        for k in range(8):
            side = lax.rem(core + k, 2)
            at = lax.rem((k // 2 + 4 - x) * step4, 4)
            values = full[p, side, at, s].astype(F32)
            blocks.append((values * scale * gain[0:1, 256 * k : 256 * k + 256]).astype(BF16))
        return blocks

    def product(blocks, ref):
        total = None
        for k in range(8):
            term = jnp.dot(blocks[k], shards(ref, k), preferred_element_type=F32)
            total = term if total is None else total + term
        return total

    def gate_task(s):
        both = product(normalised(0, s, mix_gain), vg)
        gated = both[:, 0:256] / (1.0 + jnp.exp(-both[:, 256:512]))
        padded[0, s, 32:160, :] = gated[:, 0:128]
        padded[1, s, 32:160, :] = gated[:, 128:256]

    def filter_task(s):
        sums, squares = 0.0, 0.0
        for tile in range(2):
            lanes = slice(128 * tile, 128 * tile + 128)
            total = jnp.zeros((LENGTH, 128), F32)
            for k in range(KWIDTH):
                total = total + taps[k : k + 1, lanes] * padded[tile, s, 2 + k : 130 + k, :]
            filtered[s, :, lanes] = total
            sums = sums + total
            squares = squares + total * total
        lane = lax.broadcasted_iota(jnp.int32, (LENGTH, 128), 1)
        table = jnp.where(
            lane == 0,
            jnp.sum(sums, axis=-1, keepdims=True),
            jnp.where(lane == 1, jnp.sum(squares, axis=-1, keepdims=True), 0.0),
        )
        stats[s] = table.T[0:8, :]

    def activate_task(s):
        total = stats[s]
        for j in range(7):
            total = total + stats_in[s, j]
        table = jnp.concatenate([total, jnp.zeros((LENGTH - 8, 128), F32)], axis=0).T
        mean = table[:, 0:1] / D
        variance = table[:, 1:2] / D - mean * mean
        scale = lax.rsqrt(variance + EPS)
        v = (filtered[s] - mean) * scale * chan_own[...]
        activated[s] = (v / (1.0 + jnp.exp(-v))).astype(BF16)

    def term(left, ref, towards, which):
        there = lax.rem(x + towards * step4, 4)
        right = shards(ref, there * 2 + which)
        return lax.dot_general(left, right, (((1,), (1,)), ((), ())), preferred_element_type=F32)

    def sibling_task(p, s, left, ref):
        rows = left[s]
        for m in range(4):
            to_sibling[p, s, (4 - m) % 4] = term(rows, ref, m, 1 - core).astype(BF16)

    def own_task(p, s, left, ref):
        rows = left[s]
        direct, later = (3, 1) if s in FORWARD_SEQS else (1, 3)
        for m in (2, direct, later, 0):
            total = term(rows, ref, m, core) + from_sibling[p, s, m].astype(F32)
            if m == 2:
                sent[p, s, 0] = total.astype(BF16)
            elif m == direct:
                sent[p, s, 1] = total.astype(BF16)
            elif m == later:
                relay_part[p, s] = total
            else:
                kept[p, s] = total

    def relay_task(p, s):
        sent[p, s, 2] = (relay_part[p, s] + relayed[p, s].astype(F32)).astype(BF16)

    def total_of(p, s):
        return kept[p, s] + arrived[p, s, 0].astype(F32) + arrived[p, s, 1].astype(F32)

    def middle_task(s):
        full[1, 0, 0, s] = (full[0, 0, 0, s].astype(F32) + total_of(0, s)).astype(BF16)

    def out_task(s):
        result = full[1, 0, 0, s].astype(F32) + total_of(1, s)
        out[LENGTH * s : LENGTH * s + LENGTH, :] = result.astype(BF16)

    def up_task(s):
        upward = jnp.maximum(product(normalised(1, s, mlp_gain), up), 0.0)
        hidden[s] = (upward * upward).astype(BF16)

    for s in range(SEQS):
        plan.task(f"gate{s}", functools.partial(gate_task, s), complete["vg"] | set(gathered[0, s]), 1.0, 50 + s)
        plan.task(f"filter{s}", functools.partial(filter_task, s), [f"gate{s}"], 1.0, 40 + s)
        names = []
        for j in range(1, 8):
            names.append(f"t{s}{j}")
            plan.copy(
                names[-1], stats.at[s], stats_in.at[s, j - 1], {"tp": lax.rem(tp + j, 8)}, "t", [f"filter{s}"], 0
            )
        plan.task(f"act{s}", functools.partial(activate_task, s), names, 0.5, 35 + s)
    for p, (ref, left, weight) in enumerate(((mx, activated, "mx"), (dn, hidden, "dn"))):
        for s in range(SEQS):
            if p == 1:
                plan.task(
                    f"up{s}", functools.partial(up_task, s), complete["up"] | set(gathered[1, s]), 1.2, 25 + s
                )
            source = f"up{s}" if p else f"act{s}"
            name = f"r{p}{s}"
            time = 1.2 if p else 0.6
            plan.task(
                f"{name}sib", functools.partial(sibling_task, p, s, left, ref), complete[weight] | {source}, time, 20 + s
            )
            plan.copy(f"{name}D", to_sibling.at[p, s], from_sibling.at[p, s], sibling, "d", [f"{name}sib"], 0)
            plan.task(f"{name}own", functools.partial(own_task, p, s, left, ref), [f"{name}D"], time, 15 + s)
            ahead = s in FORWARD_SEQS
            towards, link = (x_ahead, "xF") if ahead else (x_back, "xR")
            other, other_link = (x_back, "xR") if ahead else (x_ahead, "xF")
            plan.copy(f"{name}L", sent.at[p, s, 0], relayed.at[p, s], towards, link, [f"{name}own"], 0)
            plan.copy(f"{name}E", sent.at[p, s, 1], arrived.at[p, s, 0], other, other_link, [f"{name}own"], 1)
            plan.task(f"{name}rel", functools.partial(relay_task, p, s), [f"{name}L", f"{name}own"], 0.1, 5 + s)
            plan.copy(f"{name}M", sent.at[p, s, 2], arrived.at[p, s, 1], towards, link, [f"{name}rel"], 0)
            last = functools.partial(out_task if p else middle_task, s)
            plan.task(f"out{s}" if p else f"mid{s}", last, [f"{name}E", f"{name}M"], 0.2, s)
    plan.emit()


COPIES = 4 * 29 + 2 * SEQS * 7 + SEQS * 7 + 2 * SEQS * 4


def body(states, mix_gain, w_value, w_gate, conv_kernel, chan_gain, w_mix_out, mlp_gain, w_up, w_down_t):
    anywhere = pl.BlockSpec(memory_space=pl.ANY)
    vmem = pl.BlockSpec(memory_space=pltpu.VMEM)
    block = (LENGTH, 256)
    return pl.pallas_call(
        kernel,
        name="layer",
        out_shape=jax.ShapeDtypeStruct((SEQS * LENGTH, 256), BF16),
        in_specs=[anywhere] * 8 + [vmem] * 2,
        out_specs=vmem,
        scratch_shapes=[
            *[pltpu.VMEM((8, 4, 64, TENSORS[name][0]), BF16) for name in ("vg", "mx", "up", "dn")],
            pltpu.VMEM((2, 2, 4, SEQS, *block), BF16),
            pltpu.VMEM((KWIDTH, 256), F32),
            pltpu.VMEM((1, 256), F32),
            pltpu.VMEM((2, SEQS, 160, 128), F32),
            pltpu.VMEM((SEQS, *block), F32),
            pltpu.VMEM((SEQS, 8, 128), F32),
            pltpu.VMEM((SEQS, 7, 8, 128), F32),
            pltpu.VMEM((SEQS, *block), BF16),
            pltpu.VMEM((SEQS, LENGTH, 768), BF16),
            pltpu.VMEM((2, SEQS, 4, *block), BF16),
            pltpu.VMEM((2, SEQS, 4, *block), BF16),
            pltpu.VMEM((2, SEQS, *block), F32),
            pltpu.VMEM((2, SEQS, 3, *block), BF16),
            pltpu.VMEM((2, SEQS, *block), F32),
            pltpu.VMEM((2, SEQS, *block), BF16),
            pltpu.VMEM((2, SEQS, 2, *block), BF16),
            pltpu.SemaphoreType.DMA((8,)),
            pltpu.SemaphoreType.DMA((COPIES,)),
            pltpu.SemaphoreType.DMA((COPIES,)),
        ],
        compiler_params=pltpu.CompilerParams(
            collective_id=0, has_side_effects=True, vmem_limit_bytes=48 * 1024 * 1024
        ),
    )(
        states.reshape(SEQS, *block), w_value, w_gate, w_mix_out, w_up, w_down_t, conv_kernel,
        chan_gain.reshape(1, D), mix_gain.reshape(1, D), mlp_gain.reshape(1, D),
    )


def solution(mesh):
    return jax.shard_map(
        body,
        mesh=mesh,
        in_specs=(
            P(("rep", "fs"), "tp"),
            P(),
            P("fs", "tp"),
            P("fs", "tp"),
            P(),
            P(),
            P("fs", "tp"),
            P(),
            P("fs", "tp"),
            P("fs", "tp"),
        ),
        out_specs=P(("rep", "fs"), "tp"),
        check_vma=False,
    )
```

```python
import functools

import jax
import jax.numpy as jnp
from jax import lax
from jax.experimental import pallas as pl
from jax.experimental.pallas import tpu as pltpu
from jax.sharding import PartitionSpec as P

D = 2048
KWIDTH = 31
LENGTH = 128
SEQS = 3
EPS = 1e-06
F32 = jnp.float32
BF16 = jnp.bfloat16

EIGHT = ((0, 1), (7, 8), (1, 2), (6, 7), (2, 3), (5, 6), (3, 4), (4, 5))
FOUR = ((0, 1), (6, 8), (1, 3), (3, 6))
TENSORS = {
    "vg": (512, 32, EIGHT, (0, 2, 4, 6), (0, 1, 2, 3, 4)),
    "mx": (256, 32, FOUR, (0, 3), (0, 2, 4)),
    "up": (768, 48, EIGHT, (0, 2, 4, 6), (0, 2, 4)),
    "dn": (768, 32, FOUR, (0, 3), (0, 1, 2, 3, 4)),
}

RATE = 46600.0
SIBLING_RATE = 300000.0
HOP = 3.2
SIBLING_HOP = 1.0
WINDOW = 1.0


class Plan:
    def __init__(self, send_sems, recv_sems):
        self.copies, self.tasks = {}, {}
        self.send_sems, self.recv_sems = send_sems, recv_sems

    def copy(self, name, src, dst, device, links, needs=()):
        index = len(self.copies)
        size = 2 if src.dtype == BF16 else 4
        for extent in src.shape:
            size *= extent
        descriptor = pltpu.make_async_remote_copy(
            src_ref=src,
            dst_ref=dst,
            send_sem=self.send_sems.at[index],
            recv_sem=self.recv_sems.at[index],
            device_id=device,
            device_id_type=pl.DeviceIdType.MESH,
        )
        took, hop = (size / SIBLING_RATE, SIBLING_HOP) if links == ("d",) else (size / RATE, HOP)
        self.copies[name] = (descriptor, links, took, hop, frozenset(needs))

    def task(self, name, fn, needs, time):
        self.tasks[name] = (fn, frozenset(needs), time)

    def tails(self):
        own = {n: took + hop for n, (_, _, took, hop, _) in self.copies.items()}
        own.update({n: time for n, (_, _, time) in self.tasks.items()})
        users = {n: [] for n in own}
        for table in (self.copies, self.tasks):
            for n, entry in table.items():
                for need in entry[-1] if table is self.copies else entry[1]:
                    users[need].append(n)
        tails = {}

        def tail(n):
            if n not in tails:
                tails[n] = own[n] + max((tail(u) for u in users[n]), default=0.0)
            return tails[n]

        for n in own:
            tail(n)
        return tails

    def emit(self):
        now, done, free = 0.0, set(), {}
        tails = self.tails()
        arrives, tasks = {}, dict(self.tasks)
        order = sorted(self.copies, key=lambda n: -tails[n])
        waiting = {n: self.copies[n] for n in order}
        while waiting or arrives or tasks:
            later = []
            for name in list(waiting):
                descriptor, links, took, hop, needs = waiting[name]
                if not needs <= done:
                    continue
                busy = max(free.get(link, 0.0) for link in links)
                if busy - now < WINDOW:
                    for link in links:
                        free[link] = max(free.get(link, 0.0), now) + took
                    arrives[name] = max(free[link] for link in links) + hop
                    descriptor.start()
                    del waiting[name]
                else:
                    later.append(busy - WINDOW + 0.001)
            here = [n for n in arrives if arrives[n] <= now]
            if here:
                first = min(here, key=lambda n: arrives[n])
                self.copies[first][0].wait_recv()
                del arrives[first]
                done.add(first)
                now += 0.02
                continue
            ready = [n for n in tasks if tasks[n][1] <= done]
            if ready:
                best = max(ready, key=lambda n: tails[n])
                fn, _, time = tasks.pop(best)
                fn()
                done.add(best)
                now += time
                continue
            now = max(now, min(later + list(arrives.values()))) + 1e-6
        for descriptor, *_ in self.copies.values():
            descriptor.wait_send()
        return now


def kernel(
    states, w_value, w_gate, w_mix, w_up, w_down, conv, chan, mix_hbm, mlp_hbm, out,
    vg, mx, up, dn, full, taps, chan_own, padded, filtered, stats, stats_in, activated, hidden,
    to_sibling, from_sibling, kept, sent, arrived, mix_gain, mlp_gain,
    local_sems, send_sems, recv_sems,
):
    rep, fs, tp = lax.axis_index("rep"), lax.axis_index("fs"), lax.axis_index("tp")
    y, z_lo = lax.rem(fs, 8), fs // 8
    z = rep * 4 + z_lo
    x, core = tp // 2, lax.rem(tp, 2)
    step8, step4 = 1 + 6 * core, 1 + 2 * core

    def y_to(hops):
        return {"fs": z_lo * 8 + lax.rem(y + hops * step8, 8)}

    def z_to(hops):
        there = lax.rem(z + hops * step8, 8)
        return {"rep": there // 4, "fs": lax.rem(there, 4) * 8 + y}

    def x_to(hops):
        return {"tp": lax.rem(x + hops * step4, 4) * 2 + core}

    y_ahead, y_back, z_ahead, z_back = y_to(1), y_to(7), z_to(1), z_to(7)
    x_ahead, x_across, x_back = x_to(1), x_to(2), x_to(3)
    sibling = {"tp": tp + 1 - 2 * core}

    own = pl.ds(pl.multiple_of(tp * 256, 256), 256)
    loads = [
        (states, full.at[0, 0, 0]),
        (w_value, vg.at[0, 0, :, 0:256]),
        (w_gate, vg.at[0, 0, :, 256:512]),
        (w_mix, mx.at[0, 0]),
        (w_up, up.at[0, 0]),
        (w_down, dn.at[0, 0]),
        (conv.at[:, own], taps),
        (chan.at[:, own], chan_own),
        (mix_hbm, mix_gain),
        (mlp_hbm, mlp_gain),
    ]
    loads = [pltpu.make_async_copy(a, b, local_sems.at[i]) for i, (a, b) in enumerate(loads)]
    for load in loads:
        load.start()

    barrier = pltpu.get_barrier_semaphore()
    peers = [y_ahead, y_back, z_ahead, z_back]
    peers += [{"tp": lax.rem(tp + j, 8)} for j in range(1, 8)]
    for peer in peers:
        pl.semaphore_signal(
            barrier, inc=1, device_id=peer, device_id_type=pl.DeviceIdType.MESH
        )
    for tile in range(2):
        for s in range(SEQS):
            padded[tile, s, 0:32, :] = jnp.zeros((32, 128), F32)
    for load in loads:
        load.wait()
    pl.semaphore_wait(barrier, len(peers))

    plan = Plan(send_sems, recv_sems)

    complete = {}
    for name, ref in (("vg", vg), ("mx", mx), ("up", up), ("dn", dn)):
        _, cut, groups, forward, cuts = TENSORS[name]
        before = set(plan.copies)
        low, high = pl.ds(0, cut), pl.ds(cut, 64 - cut)
        for d in range(1, 5):
            needs = [f"{name}y{9 - d}"] if d > 1 else []
            plan.copy(f"{name}y{8 - d}", ref.at[(9 - d) % 8, 0, low], ref.at[8 - d, 0, low], y_ahead, ("yF",), needs)
        for d in range(1, 4):
            needs = [f"{name}y{d - 1}"] if d > 1 else []
            plan.copy(f"{name}y{d}", ref.at[d - 1, 0, low], ref.at[d, 0, low], y_back, ("yR",), needs)
        for g, (lo, hi) in enumerate(groups):
            rows = pl.ds(lo, hi - lo)
            needs = [f"{name}y{m}" for m in range(lo, hi) if m]
            plan.copy(f"{name}zF{g}", ref.at[rows, 0, low], ref.at[rows, 3, low], z_ahead, ("zF",), needs)
            plan.copy(f"{name}zR{g}", ref.at[rows, 0, low], ref.at[rows, 1, low], z_back, ("zR",), needs)
            if g in forward:
                plan.copy(f"{name}zX{g}", ref.at[rows, 3, low], ref.at[rows, 2, low], z_ahead, ("zF",), [f"{name}zF{g}"])
            else:
                plan.copy(f"{name}zX{g}", ref.at[rows, 1, low], ref.at[rows, 2, low], z_back, ("zR",), [f"{name}zR{g}"])
        plan.copy(f"{name}b3", ref.at[0, 0, high], ref.at[0, 3, high], z_ahead, ("zF",))
        plan.copy(f"{name}b1", ref.at[0, 0, high], ref.at[0, 1, high], z_back, ("zR",))
        plan.copy(f"{name}b2", ref.at[0, 3, high], ref.at[0, 2, high], z_ahead, ("zF",), [f"{name}b3"])
        for i, (lo, hi) in enumerate(zip(cuts, cuts[1:])):
            at_z = pl.ds(lo, hi - lo)
            first = [f"{name}b{m}" for m in range(lo, hi) if m]
            for d in range(1, 5):
                needs = [f"{name}c{i}{9 - d}"] if d > 1 else first
                plan.copy(
                    f"{name}c{i}{8 - d}", ref.at[(9 - d) % 8, at_z, high], ref.at[8 - d, at_z, high], y_ahead, ("yF",), needs
                )
            for d in range(1, 4):
                needs = [f"{name}c{i}{d - 1}"] if d > 1 else first
                plan.copy(
                    f"{name}c{i}{d}", ref.at[d - 1, at_z, high], ref.at[d, at_z, high], y_back, ("yR",), needs
                )
        complete[name] = set(plan.copies) - before

    def shards(ref, block):
        at_z = lax.rem((block // 2 + 4 - z_lo) * step4, 4)
        pieces = []
        for i in range(4):
            at_y = lax.rem((lax.rem(block, 2) * 4 + i + 8 - y) * step8, 8)
            pieces.append(ref[at_y, at_z])
        return jnp.concatenate(pieces, axis=0)

    gathered = {}
    for p in range(2):
        for s in range(SEQS):
            rows = full.at[p]
            needs = [f"mid{s}"] if p else []
            name = f"g{p}{s}"
            mine = rows.at[0, 0, s]
            plan.copy(f"{name}3", mine, rows.at[0, 3, s], x_ahead, ("xF",), needs)
            plan.copy(f"{name}1", mine, rows.at[0, 1, s], x_back, ("xR",), needs)
            plan.copy(f"{name}2", mine, rows.at[0, 2, s], x_across, ("xF", "xR"), needs)
            plan.copy(f"{name}S0", mine, rows.at[1, 0, s], sibling, ("d",), needs)
            for m in (1, 2, 3):
                plan.copy(f"{name}S{m}", rows.at[0, m, s], rows.at[1, 4 - m, s], sibling, ("d",), [f"{name}{m}"])
            gathered[p, s] = [name + k for k in ("3", "1", "2", "S0", "S1", "S2", "S3")]

    def normalised(p, s, gain):
        squares = jnp.zeros((LENGTH, 256), F32)
        for side in range(2):
            for at in range(4):
                values = full[p, side, at, s].astype(F32)
                squares = squares + values * values
        scale = lax.rsqrt(jnp.sum(squares, axis=-1, keepdims=True) / D + EPS)
        blocks = []
        for k in range(8):
            side = lax.rem(core + k, 2)
            at = lax.rem((k // 2 + 4 - x) * step4, 4)
            values = full[p, side, at, s].astype(F32)
            blocks.append((values * scale * gain[0:1, 256 * k : 256 * k + 256]).astype(BF16))
        return blocks

    def product(blocks, ref):
        total = None
        for k in range(8):
            term = jnp.dot(blocks[k], shards(ref, k), preferred_element_type=F32)
            total = term if total is None else total + term
        return total

    def gate_task(s):
        both = product(normalised(0, s, mix_gain), vg)
        gated = both[:, 0:256] / (1.0 + jnp.exp(-both[:, 256:512]))
        padded[0, s, 32:160, :] = gated[:, 0:128]
        padded[1, s, 32:160, :] = gated[:, 128:256]

    def filter_task(s):
        sums, squares = 0.0, 0.0
        for tile in range(2):
            lanes = slice(128 * tile, 128 * tile + 128)
            total = jnp.zeros((LENGTH, 128), F32)
            for k in range(KWIDTH):
                total = total + taps[k : k + 1, lanes] * padded[tile, s, 2 + k : 130 + k, :]
            filtered[s, :, lanes] = total
            sums = sums + total
            squares = squares + total * total
        lane = lax.broadcasted_iota(jnp.int32, (LENGTH, 128), 1)
        table = jnp.where(
            lane == 0,
            jnp.sum(sums, axis=-1, keepdims=True),
            jnp.where(lane == 1, jnp.sum(squares, axis=-1, keepdims=True), 0.0),
        )
        stats[s] = table.T[0:8, :]

    def activate_task(s):
        total = stats[s]
        for j in range(7):
            total = total + stats_in[s, j]
        table = jnp.concatenate([total, jnp.zeros((LENGTH - 8, 128), F32)], axis=0).T
        mean = table[:, 0:1] / D
        variance = table[:, 1:2] / D - mean * mean
        scale = lax.rsqrt(variance + EPS)
        v = (filtered[s] - mean) * scale * chan_own[...]
        activated[s] = (v / (1.0 + jnp.exp(-v))).astype(BF16)

    def term(left, ref, towards, which):
        there = lax.rem(x + towards * step4, 4)
        right = shards(ref, there * 2 + which)
        return lax.dot_general(left, right, (((1,), (1,)), ((), ())), preferred_element_type=F32)

    def sibling_task(p, s, left, ref):
        rows = left[s]
        for m in range(4):
            to_sibling[p, s, (4 - m) % 4] = term(rows, ref, m, 1 - core).astype(BF16)

    def own_task(p, s, left, ref):
        rows = left[s]
        for m in (2, 1, 3, 0):
            total = term(rows, ref, m, core) + from_sibling[p, s, m].astype(F32)
            if m:
                sent[p, s, m - 1] = total.astype(BF16)
            else:
                kept[p, s] = total

    def total_of(p, s):
        total = kept[p, s]
        for m in range(3):
            total = total + arrived[p, s, m].astype(F32)
        return total

    def middle_task(s):
        full[1, 0, 0, s] = (full[0, 0, 0, s].astype(F32) + total_of(0, s)).astype(BF16)

    def out_task(s):
        result = full[1, 0, 0, s].astype(F32) + total_of(1, s)
        out[LENGTH * s : LENGTH * s + LENGTH, :] = result.astype(BF16)

    def up_task(s):
        upward = jnp.maximum(product(normalised(1, s, mlp_gain), up), 0.0)
        hidden[s] = (upward * upward).astype(BF16)

    for s in range(SEQS):
        plan.task(f"gate{s}", functools.partial(gate_task, s), complete["vg"] | set(gathered[0, s]), 0.4)
        plan.task(f"filter{s}", functools.partial(filter_task, s), [f"gate{s}"], 0.6)
        names = []
        for j in range(1, 8):
            names.append(f"t{s}{j}")
            peer = {"tp": lax.rem(tp + j, 8)}
            plan.copy(names[-1], stats.at[s], stats_in.at[s, j - 1], peer, ("t",), [f"filter{s}"])
        plan.task(f"act{s}", functools.partial(activate_task, s), names, 0.3)
    for p, (ref, left, weight) in enumerate(((mx, activated, "mx"), (dn, hidden, "dn"))):
        for s in range(SEQS):
            if p == 1:
                plan.task(f"up{s}", functools.partial(up_task, s), complete["up"] | set(gathered[1, s]), 0.5)
            source = f"up{s}" if p else f"act{s}"
            name = f"r{p}{s}"
            time = 0.5 if p else 0.25
            plan.task(f"{name}sib", functools.partial(sibling_task, p, s, left, ref), complete[weight] | {source}, time)
            plan.copy(f"{name}D", to_sibling.at[p, s], from_sibling.at[p, s], sibling, ("d",), [f"{name}sib"])
            plan.task(f"{name}own", functools.partial(own_task, p, s, left, ref), [f"{name}D"], time)
            routes = ((x_ahead, ("xF",)), (x_across, ("xF", "xR")), (x_back, ("xR",)))
            for m, (peer, links) in enumerate(routes):
                plan.copy(f"{name}{m}", sent.at[p, s, m], arrived.at[p, s, m], peer, links, [f"{name}own"])
            last = functools.partial(out_task if p else middle_task, s)
            plan.task(f"out{s}" if p else f"mid{s}", last, [f"{name}{m}" for m in range(3)], 0.2)
    plan.emit()


COPIES = sum(7 + 3 * len(groups) + 3 + 7 * (len(cuts) - 1) for _, _, groups, _, cuts in TENSORS.values())
COPIES += 2 * SEQS * 7 + SEQS * 7 + 2 * SEQS * 4


def body(states, mix_gain, w_value, w_gate, conv_kernel, chan_gain, w_mix_out, mlp_gain, w_up, w_down_t):
    anywhere = pl.BlockSpec(memory_space=pltpu.HBM)
    vmem = pl.BlockSpec(memory_space=pltpu.VMEM)
    block = (LENGTH, 256)
    return pl.pallas_call(
        kernel,
        name="layer",
        out_shape=jax.ShapeDtypeStruct((SEQS * LENGTH, 256), BF16),
        in_specs=[anywhere] * 10,
        out_specs=vmem,
        scratch_shapes=[
            *[pltpu.VMEM((8, 4, 64, TENSORS[name][0]), BF16) for name in ("vg", "mx", "up", "dn")],
            pltpu.VMEM((2, 2, 4, SEQS, *block), BF16),
            pltpu.VMEM((KWIDTH, 256), F32),
            pltpu.VMEM((1, 256), F32),
            pltpu.VMEM((2, SEQS, 160, 128), F32),
            pltpu.VMEM((SEQS, *block), F32),
            pltpu.VMEM((SEQS, 8, 128), F32),
            pltpu.VMEM((SEQS, 7, 8, 128), F32),
            pltpu.VMEM((SEQS, *block), BF16),
            pltpu.VMEM((SEQS, LENGTH, 768), BF16),
            pltpu.VMEM((2, SEQS, 4, *block), BF16),
            pltpu.VMEM((2, SEQS, 4, *block), BF16),
            pltpu.VMEM((2, SEQS, *block), F32),
            pltpu.VMEM((2, SEQS, 3, *block), BF16),
            pltpu.VMEM((2, SEQS, 3, *block), BF16),
            pltpu.VMEM((1, D), F32),
            pltpu.VMEM((1, D), F32),
            pltpu.SemaphoreType.DMA((10,)),
            pltpu.SemaphoreType.DMA((COPIES,)),
            pltpu.SemaphoreType.DMA((COPIES,)),
        ],
        compiler_params=pltpu.CompilerParams(
            collective_id=0, has_side_effects=True, vmem_limit_bytes=67043328
        ),
    )(
        states.reshape(SEQS, *block), w_value, w_gate, w_mix_out, w_up, w_down_t, conv_kernel,
        chan_gain.reshape(1, D), mix_gain.reshape(1, D), mlp_gain.reshape(1, D),
    )


def solution(mesh):
    return jax.shard_map(
        body,
        mesh=mesh,
        in_specs=(
            P(("rep", "fs"), "tp"),
            P(),
            P("fs", "tp"),
            P("fs", "tp"),
            P(),
            P(),
            P("fs", "tp"),
            P(),
            P("fs", "tp"),
            P("fs", "tp"),
        ),
        out_specs=P(("rep", "fs"), "tp"),
        check_vma=False,
    )
```

```python
import functools

import jax
import jax.numpy as jnp
from jax import lax
from jax.experimental import pallas as pl
from jax.experimental.pallas import tpu as pltpu
from jax.sharding import PartitionSpec as P

D = 2048
KWIDTH = 31
LENGTH = 128
SEQS = 3
EPS = 1e-06
F32 = jnp.float32
BF16 = jnp.bfloat16

EIGHT = ((0, 1), (7, 8), (1, 2), (6, 7), (2, 3), (5, 6), (3, 4), (4, 5))
FOUR = ((0, 1), (6, 8), (1, 3), (3, 6))


class Way:
    def __init__(self, rows, cut, groups, relay, y, c, far, direct, cuts, bias):
        self.low, self.high = rows
        self.cut, self.groups, self.relay = cut, groups, relay
        self.y, self.c, self.far, self.direct, self.cuts, self.bias = y, c, far, direct, cuts, bias


COLUMNS = {"vg": 512, "mx": 256, "up": 768, "dn": 768}
WAYS = {
    "vg": Way((0, 64), 32, EIGHT, "FRRFFRRF", "ring", "ring", "FFFRRR", True, (0, 1, 2, 3, 4), 2.0),
    "mx": Way((0, 64), 40, FOUR, "FRRF", "ring", "ring", "FFFRRR", True, (0, 2, 4), 2.0),
    "up": Way((0, 64), 48, EIGHT, "FRRFFRRF", "ring", "ring", "FRRFRF", False, (0, 2, 4), 0.0),
    "dn": Way((0, 32), 16, FOUR, "FRRF", "ring", "ring", "FFRFRF", False, (0, 4), 2.0),
    "dm": Way((32, 64), 16, FOUR, "FRRF", "ring", "ring", "FRRFFF", False, (0, 2, 4), -2.0),
}
X_GATHER = ('RRD', 'DRD')
X_SUM = ('RDD', 'DRF')

RATE = 46600.0
SIBLING_RATE = 300000.0
HOP = 3.2
FURTHER_HOP = 0.5
SIBLING_HOP = 1.0
PER_COPY = 0.08
SEND_SLACK = 3.0
WINDOW = 0.3


OPPOSITE = {"y1": "y7", "y7": "y1", "y2": "y6", "y6": "y2", "z1": "z7", "z7": "z1", "x1": "x3", "x3": "x1", "x2": "x2", "d": "d"}


class Plan:
    def __init__(self, send_sems, recv_sems):
        self.copies, self.tasks, self.bias = {}, {}, {}
        self.send_sems, self.recv_sems = send_sems, recv_sems

    def copy(self, name, src, dst, device, links, needs=(), hops=1, along=1, bias=0.0):
        size = 2 if src.dtype == BF16 else 4
        for extent in src.shape:
            size *= extent
        if links == ("d",):
            took, hop = size / SIBLING_RATE, SIBLING_HOP
        else:
            took, hop = size * along / RATE, HOP + FURTHER_HOP * (hops - 1)
        self.copies[name] = ((src, dst, *device), links, took + PER_COPY, hop, frozenset(needs))
        self.bias[name] = bias

    def task(self, name, fn, needs, time):
        self.tasks[name] = (fn, frozenset(needs), time)

    def tails(self):
        own = {n: took + hop for n, (_, _, took, hop, _) in self.copies.items()}
        own.update({n: time for n, (_, _, time) in self.tasks.items()})
        users = {n: [] for n in own}
        for table in (self.copies, self.tasks):
            for n, entry in table.items():
                for need in entry[-1] if table is self.copies else entry[1]:
                    users[need].append(n)
        tails = {}

        def tail(n):
            if n not in tails:
                tails[n] = own[n] + max((tail(u) for u in users[n]), default=0.0)
            return tails[n]

        for n in own:
            tail(n)
        return tails

    def emit(self):
        now, step, done, free = 0.0, 0, set(), {}
        tails = self.tails()
        arrives, tasks = {}, dict(self.tasks)
        order = sorted(self.copies, key=lambda n: -tails[n] - self.bias[n])
        waiting = {n: self.copies[n] for n in order}
        started, started_at, heard, sends, receives, n_sends = {}, {}, {}, [], [], 0
        while waiting or arrives or tasks:
            later = []
            for name in list(waiting):
                (src, dst, where, device), links, took, hop, needs = waiting[name]
                if not needs <= done:
                    continue
                busy = max(free.get(link, 0.0) for link in links)
                if busy - now < WINDOW:
                    for link in links:
                        free[link] = max(free.get(link, 0.0), now) + took
                    left = max(free[link] for link in links)
                    arrives[name] = left + hop
                    if sends and sends[0][0] + SEND_SLACK < now:
                        _, send, last = sends.pop(0)
                        last.wait_send()
                    else:
                        send, n_sends = n_sends, n_sends + 1
                    known = heard.get(OPPOSITE.get(where), -1)
                    receive = next((r for r, at in enumerate(receives) if at < known), len(receives))
                    receives[receive : receive + 1] = [1 << 30]
                    step += 1
                    started_at[name] = step
                    descriptor = pltpu.make_async_remote_copy(
                        src_ref=src,
                        dst_ref=dst,
                        send_sem=self.send_sems.at[send],
                        recv_sem=self.recv_sems.at[receive],
                        device_id=device,
                        device_id_type=pl.DeviceIdType.MESH,
                    )
                    descriptor.start()
                    started[name] = descriptor, where, receive
                    sends.append((left, send, descriptor))
                    sends.sort(key=lambda entry: entry[:2])
                    del waiting[name]
                else:
                    later.append(busy - WINDOW + 0.001)
            here = [n for n in arrives if arrives[n] <= now]
            if here:
                first = min(here, key=lambda n: arrives[n])
                descriptor, where, receive = started.pop(first)
                descriptor.wait_recv()
                step += 1
                receives[receive] = step
                heard[where] = max(heard.get(where, -1), started_at[first])
                del arrives[first]
                done.add(first)
                now += 0.02
                continue
            ready = [n for n in tasks if tasks[n][1] <= done]
            if ready:
                best = max(ready, key=lambda n: tails[n])
                fn, _, time = tasks.pop(best)
                fn()
                done.add(best)
                now += time
                continue
            now = max(now, min(later + list(arrives.values()))) + 1e-6
        for _, _, descriptor in sends:
            descriptor.wait_send()
        assert n_sends <= SEND_SEMS and len(receives) <= RECEIVE_SEMS, (n_sends, len(receives))
        return now


def kernel(
    states, w_value, w_gate, w_mix, w_up, w_down, conv, chan, mix_hbm, mlp_hbm, out,
    vg, mx, up, dn, full, taps, chan_own, padded, filtered, stats, stats_in, activated, hidden,
    mix_gain, mlp_gain, local_sems, send_sems, recv_sems, *buffers,
):
    rep, fs, tp = lax.axis_index("rep"), lax.axis_index("fs"), lax.axis_index("tp")
    y, z_lo = lax.rem(fs, 8), fs // 8
    z = rep * 4 + z_lo
    x, core = tp // 2, lax.rem(tp, 2)
    step8, step4 = 1 + 6 * core, 1 + 2 * core

    def y_to(hops):
        return f"y{hops}", {"fs": z_lo * 8 + lax.rem(y + hops * step8, 8)}

    def z_to(hops):
        there = lax.rem(z + hops * step8, 8)
        return f"z{hops}", {"rep": there // 4, "fs": lax.rem(there, 4) * 8 + y}

    def x_to(hops):
        return f"x{hops}", {"tp": lax.rem(x + hops * step4, 4) * 2 + core}

    y_ahead, y_back, z_ahead, z_back, z_across = y_to(1), y_to(7), z_to(1), z_to(7), z_to(2)
    x_ahead, x_across, x_back = x_to(1), x_to(2), x_to(3)
    sibling = "d", {"tp": tp + 1 - 2 * core}

    own = pl.ds(pl.multiple_of(tp * 256, 256), 256)
    loads = [
        (states, full.at[0, 0, 0]),
        (w_value, vg.at[0, 0, :, 0:256]),
        (w_gate, vg.at[0, 0, :, 256:512]),
        (w_mix, mx.at[0, 0]),
        (w_up, up.at[0, 0]),
        (w_down, dn.at[0, 0]),
        (conv.at[:, own], taps),
        (chan.at[:, own], chan_own),
        (mix_hbm, mix_gain),
        (mlp_hbm, mlp_gain),
    ]
    loads = [pltpu.make_async_copy(a, b, local_sems.at[i]) for i, (a, b) in enumerate(loads)]
    for load in loads:
        load.start()

    barrier = pltpu.get_barrier_semaphore()
    peers = [y_ahead, y_back, z_ahead, z_back]
    if any(way.y != "ring" or way.c != "ring" for way in WAYS.values()):
        peers += [y_to(2), y_to(6)]
    if any(way.direct or "D" in way.relay for way in WAYS.values()):
        peers += [z_across, z_to(6)]
    peers += [("tp", {"tp": lax.rem(tp + j, 8)}) for j in range(1, 8)]
    for _, peer in peers:
        pl.semaphore_signal(
            barrier, inc=1, device_id=peer, device_id_type=pl.DeviceIdType.MESH
        )
    for tile in range(2):
        for s in range(SEQS):
            padded[tile, s, 0:32, :] = jnp.zeros((32, 128), F32)
    for load in loads:
        load.wait()
    pl.semaphore_wait(barrier, len(peers))

    plan = Plan(send_sems, recv_sems)
    wide, narrow = buffers[:7], buffers[7:]

    def along_y(name, block, how, first, far, bias):
        steps = {"F": [(8 - d, (9 - d) % 8) for d in range(1, 4)], "R": [(d, d - 1) for d in range(1, 4)]}
        if how == "ring":
            steps[far].append((4, 5) if far == "F" else (4, 3))
        for way, (link, near, over) in {"F": ("yF", y_ahead, y_to(2)), "R": ("yR", y_back, y_to(6))}.items():
            for m, before in steps[way]:
                if how == "two" and m in (2, 6):
                    plan.copy(f"{name}{m}", block(0), block(m), over, (link,), first, 2, 2, bias)
                else:
                    needs = [f"{name}{before}"] if before else first
                    plan.copy(f"{name}{m}", block(before), block(m), near, (link,), needs, bias=bias)
            if how != "ring" and way == far:
                m = 6 if far == "F" else 2
                plan.copy(f"{name}4", block(m), block(4), over, (link,), [f"{name}{m}"], 2, 2, bias)

    complete = {}
    for name, way in WAYS.items():
        ref = {"vg": vg, "mx": mx, "up": up}.get(name, dn)
        before = set(plan.copies)
        bias = way.bias
        low = pl.ds(way.low, way.cut)
        high = pl.ds(way.low + way.cut, way.high - way.low - way.cut)
        along_y(f"{name}y", lambda m, ref=ref, low=low: ref.at[m, 0, low], way.y, [], way.far[0], bias)
        for g, (lo, hi) in enumerate(way.groups):
            block = [ref.at[pl.ds(lo, hi - lo), m, low] for m in range(4)]
            needs = [f"{name}y{m}" for m in range(lo, hi) if m]
            plan.copy(f"{name}zF{g}", block[0], block[3], z_ahead, ("zF",), needs, bias=bias)
            plan.copy(f"{name}zR{g}", block[0], block[1], z_back, ("zR",), needs, bias=bias)
            if way.relay[g] == "F":
                plan.copy(f"{name}zX{g}", block[3], block[2], z_ahead, ("zF",), [f"{name}zF{g}"], bias=bias)
            elif way.relay[g] == "R":
                plan.copy(f"{name}zX{g}", block[1], block[2], z_back, ("zR",), [f"{name}zR{g}"], bias=bias)
            else:
                plan.copy(f"{name}zX{g}", block[0], block[2], z_across, ("zF", "zR"), needs, 2, bias=bias)
        block = [ref.at[0, m, high] for m in range(4)]
        plan.copy(f"{name}b3", block[0], block[3], z_ahead, ("zF",), bias=bias)
        plan.copy(f"{name}b1", block[0], block[1], z_back, ("zR",), bias=bias)
        if way.direct:
            plan.copy(f"{name}b2", block[0], block[2], z_across, ("zF", "zR"), (), 2, bias=bias)
        elif way.far[1] == "F":
            plan.copy(f"{name}b2", block[3], block[2], z_ahead, ("zF",), [f"{name}b3"], bias=bias)
        else:
            plan.copy(f"{name}b2", block[1], block[2], z_back, ("zR",), [f"{name}b1"], bias=bias)
        for i, (lo, hi) in enumerate(zip(way.cuts, way.cuts[1:])):
            at_z = pl.ds(lo, hi - lo)
            first = [f"{name}b{m}" for m in range(lo, hi) if m]
            along_y(
                f"{name}c{i}", lambda m, ref=ref, at_z=at_z, high=high: ref.at[m, at_z, high], way.c, first, way.far[2 + i], bias
            )
        complete[name] = set(plan.copies) - before

    def shards(ref, block, lo=0, hi=64):
        at_z = lax.rem((block // 2 + 4 - z_lo) * step4, 4)
        pieces = []
        for i in range(4):
            at_y = lax.rem((lax.rem(block, 2) * 4 + i + 8 - y) * step8, 8)
            pieces.append(ref[at_y, at_z, lo:hi])
        return jnp.concatenate(pieces, axis=0)

    gathered = {}
    for p in range(2):
        for s in range(SEQS):
            rows = full.at[p]
            needs = [f"mid{s}"] if p else []
            name = f"g{p}{s}"
            mine = rows.at[0, 0, s]
            plan.copy(f"{name}3", mine, rows.at[0, 3, s], x_ahead, ("xF",), needs)
            plan.copy(f"{name}1", mine, rows.at[0, 1, s], x_back, ("xR",), needs)
            if X_GATHER[p][s] == "D":
                plan.copy(f"{name}2", mine, rows.at[0, 2, s], x_across, ("xF", "xR"), needs, 2)
            elif X_GATHER[p][s] == "F":
                plan.copy(f"{name}2", rows.at[0, 3, s], rows.at[0, 2, s], x_ahead, ("xF",), [f"{name}3"])
            else:
                plan.copy(f"{name}2", rows.at[0, 1, s], rows.at[0, 2, s], x_back, ("xR",), [f"{name}1"])
            plan.copy(f"{name}S0", mine, rows.at[1, 0, s], sibling, ("d",), needs)
            for m in (1, 2, 3):
                plan.copy(f"{name}S{m}", rows.at[0, m, s], rows.at[1, 4 - m, s], sibling, ("d",), [f"{name}{m}"])
            gathered[p, s] = [name + k for k in ("3", "1", "2", "S0", "S1", "S2", "S3")]

    def normalised(p, s, gain):
        squares = jnp.zeros((LENGTH, 256), F32)
        for side in range(2):
            for at in range(4):
                values = full[p, side, at, s].astype(F32)
                squares = squares + values * values
        scale = lax.rsqrt(jnp.sum(squares, axis=-1, keepdims=True) / D + EPS)
        blocks = []
        for k in range(8):
            side = lax.rem(core + k, 2)
            at = lax.rem((k // 2 + 4 - x) * step4, 4)
            values = full[p, side, at, s].astype(F32)
            blocks.append((values * scale * gain[0:1, 256 * k : 256 * k + 256]).astype(BF16))
        return blocks

    def product(blocks, ref):
        total = None
        for k in range(8):
            term = jnp.dot(blocks[k], shards(ref, k), preferred_element_type=F32)
            total = term if total is None else total + term
        return total

    def gate_task(s):
        both = product(normalised(0, s, mix_gain), vg)
        gated = both[:, 0:256] / (1.0 + jnp.exp(-both[:, 256:512]))
        padded[0, s, 32:160, :] = gated[:, 0:128]
        padded[1, s, 32:160, :] = gated[:, 128:256]

    def filter_task(s):
        sums, squares = 0.0, 0.0
        for tile in range(2):
            lanes = slice(128 * tile, 128 * tile + 128)
            total = jnp.zeros((LENGTH, 128), F32)
            for k in range(KWIDTH):
                total = total + taps[k : k + 1, lanes] * padded[tile, s, 2 + k : 130 + k, :]
            filtered[s, :, lanes] = total
            sums = sums + total
            squares = squares + total * total
        lane = lax.broadcasted_iota(jnp.int32, (LENGTH, 128), 1)
        table = jnp.where(
            lane == 0,
            jnp.sum(sums, axis=-1, keepdims=True),
            jnp.where(lane == 1, jnp.sum(squares, axis=-1, keepdims=True), 0.0),
        )
        stats[s] = table.T[0:8, :]

    def activate_task(s):
        total = stats[s]
        for j in range(7):
            total = total + stats_in[s, j]
        table = jnp.concatenate([total, jnp.zeros((LENGTH - 8, 128), F32)], axis=0).T
        mean = table[:, 0:1] / D
        variance = table[:, 1:2] / D - mean * mean
        scale = lax.rsqrt(variance + EPS)
        v = (filtered[s] - mean) * scale * chan_own[...]
        activated[s] = (v / (1.0 + jnp.exp(-v))).astype(BF16)

    class Sums:
        def __init__(self, name, p, s, left, ref, lo, hi, how, buffers):
            self.name, self.s, self.left, self.ref, self.lo, self.hi, self.how = name, s, left, ref, lo, hi, how
            self.to_sibling, self.from_sibling, self.kept, self.sent, self.relay_part, self.relayed, self.arrived = [
                buffer.at[p, s] for buffer in buffers
            ]
            self.width = 4 * (hi - lo)
            self.direct, self.later = {"F": (3, 1), "R": (1, 3), "D": (0, 0)}[how]

        def terms(self, which):
            rows = self.left[self.s]
            at_once = 256 // self.width
            for start in range(0, 4, at_once):
                right = []
                for m in range(start, start + at_once):
                    there = lax.rem(x + m * step4, 4)
                    right.append(shards(self.ref, there * 2 + which, self.lo, self.hi))
                right = right[0] if at_once == 1 else jnp.concatenate(right, axis=0)
                both = lax.dot_general(rows, right, (((1,), (1,)), ((), ())), preferred_element_type=F32)
                for i in range(at_once):
                    yield start + i, both[:, self.width * i : self.width * (i + 1)]

        def sibling_task(self):
            for m, term in self.terms(1 - core):
                self.to_sibling[(4 - m) % 4] = term.astype(BF16)

        def own_task(self):
            for m, term in self.terms(core):
                total = term + self.from_sibling[m].astype(F32)
                if m == 0:
                    self.kept[...] = total
                elif m == self.later:
                    self.relay_part[...] = total
                else:
                    self.sent[m - 1] = total.astype(BF16)

        def relay_task(self):
            self.sent[self.later - 1] = (self.relay_part[...] + self.relayed[...].astype(F32)).astype(BF16)

        def plan(self, needs, time):
            name = self.name
            plan.task(f"{name}sib", self.sibling_task, needs, time)
            plan.copy(f"{name}D", self.to_sibling, self.from_sibling, sibling, ("d",), [f"{name}sib"])
            plan.task(f"{name}own", self.own_task, [f"{name}D"], time)
            ends = {1: (x_ahead, ("xF",)), 2: (x_across, ("xF", "xR")), 3: (x_back, ("xR",))}
            last = []
            for m in (1, 2, 3):
                if self.later and m == 2:
                    continue
                needs = [f"{name}rel"] if m == self.later else [f"{name}own"]
                last.append(f"{name}{m}")
                plan.copy(last[-1], self.sent.at[m - 1], self.arrived.at[m - 1], *ends[m], needs, 2 if m == 2 else 1)
            if self.later:
                plan.copy(f"{name}L", self.sent.at[1], self.relayed, *ends[self.later], [f"{name}own"])
                plan.task(f"{name}rel", self.relay_task, [f"{name}L", f"{name}own"], 0.1)
            return last

        def total(self):
            total = self.kept[...]
            for m in (1, 2, 3):
                if not (self.later and m == 2):
                    total = total + self.arrived[m - 1].astype(F32)
            return total

    def middle_task(s):
        full[1, 0, 0, s] = (full[0, 0, 0, s].astype(F32) + sums[0, s][0].total()).astype(BF16)

    def out_task(s):
        parts = [part.total() for part in sums[1, s]]
        if len(parts) > 1:
            parts = [part[:, 32 * i : 32 * i + 32] for i in range(4) for part in parts]
            parts = [jnp.concatenate(parts, axis=1)]
        result = full[1, 0, 0, s].astype(F32) + parts[0]
        out[LENGTH * s : LENGTH * s + LENGTH, :] = result.astype(BF16)

    def up_task(s):
        upward = jnp.maximum(product(normalised(1, s, mlp_gain), up), 0.0)
        hidden[s] = (upward * upward).astype(BF16)

    sums = {}
    for s in range(SEQS):
        plan.task(f"gate{s}", functools.partial(gate_task, s), complete["vg"] | set(gathered[0, s]), 0.35)
        plan.task(f"filter{s}", functools.partial(filter_task, s), [f"gate{s}"], 0.35)
        names = []
        for j in range(1, 8):
            names.append(f"t{s}{j}")
            peer = f"t{j}", {"tp": lax.rem(tp + j, 8)}
            plan.copy(names[-1], stats.at[s], stats_in.at[s, j - 1], peer, ("t",), [f"filter{s}"], 2)
        plan.task(f"act{s}", functools.partial(activate_task, s), names, 0.3)
        part = Sums(f"r0{s}", 0, s, activated, mx, 0, 64, X_SUM[0][s], wide)
        sums[0, s] = [part]
        plan.task(f"mid{s}", functools.partial(middle_task, s), part.plan(complete["mx"] | {f"act{s}"}, 0.25), 0.15)
        plan.task(f"up{s}", functools.partial(up_task, s), complete["up"] | set(gathered[1, s]), 0.5)
        sums[1, s], last = [], []
        for p, name in enumerate([name for name in WAYS if name in ("dn", "dm")]):
            way = WAYS[name]
            buffers = wide if way.high - way.low == 64 else narrow
            p = 1 if buffers is wide else p
            part = Sums(f"{name}{s}", p, s, hidden, dn, way.low, way.high, X_SUM[1][s], buffers)
            sums[1, s].append(part)
            last += part.plan(complete[name] | {f"up{s}"}, 0.5 if buffers is wide else 0.3)
        plan.task(f"out{s}", functools.partial(out_task, s), last, 0.15)
    plan.emit()


SEND_SEMS, RECEIVE_SEMS = 36, 93


def sum_buffers(width):
    shapes = [((4,), BF16), ((4,), BF16), ((), F32), ((3,), BF16), ((), F32), ((), BF16), ((3,), BF16)]
    return [pltpu.VMEM((2, SEQS, *lead, LENGTH, width), dtype) for lead, dtype in shapes]


def body(states, mix_gain, w_value, w_gate, conv_kernel, chan_gain, w_mix_out, mlp_gain, w_up, w_down_t):
    anywhere = pl.BlockSpec(memory_space=pltpu.HBM)
    vmem = pl.BlockSpec(memory_space=pltpu.VMEM)
    block = (LENGTH, 256)
    return pl.pallas_call(
        kernel,
        name="layer",
        out_shape=jax.ShapeDtypeStruct((SEQS * LENGTH, 256), BF16),
        in_specs=[anywhere] * 10,
        out_specs=vmem,
        scratch_shapes=[
            *[pltpu.VMEM((8, 4, 64, COLUMNS[name]), BF16) for name in ("vg", "mx", "up", "dn")],
            pltpu.VMEM((2, 2, 4, SEQS, *block), BF16),
            pltpu.VMEM((KWIDTH, 256), F32),
            pltpu.VMEM((1, 256), F32),
            pltpu.VMEM((2, SEQS, 160, 128), F32),
            pltpu.VMEM((SEQS, *block), F32),
            pltpu.VMEM((SEQS, 8, 128), F32),
            pltpu.VMEM((SEQS, 7, 8, 128), F32),
            pltpu.VMEM((SEQS, *block), BF16),
            pltpu.VMEM((SEQS, LENGTH, 768), BF16),
            pltpu.VMEM((1, D), F32),
            pltpu.VMEM((1, D), F32),
            pltpu.SemaphoreType.DMA((10,)),
            pltpu.SemaphoreType.DMA((SEND_SEMS,)),
            pltpu.SemaphoreType.DMA((RECEIVE_SEMS,)),
            *sum_buffers(256),
            *sum_buffers(128),
        ],
        compiler_params=pltpu.CompilerParams(
            collective_id=0, has_side_effects=True, vmem_limit_bytes=67043328
        ),
    )(
        states.reshape(SEQS, *block), w_value, w_gate, w_mix_out, w_up, w_down_t, conv_kernel,
        chan_gain.reshape(1, D), mix_gain.reshape(1, D), mlp_gain.reshape(1, D),
    )


def solution(mesh):
    return jax.shard_map(
        body,
        mesh=mesh,
        in_specs=(
            P(("rep", "fs"), "tp"),
            P(),
            P("fs", "tp"),
            P("fs", "tp"),
            P(),
            P(),
            P("fs", "tp"),
            P(),
            P("fs", "tp"),
            P("fs", "tp"),
        ),
        out_specs=P(("rep", "fs"), "tp"),
        check_vma=False,
    )
```

```python
import functools

import jax
import jax.numpy as jnp
from jax import lax
from jax.experimental import pallas as pl
from jax.experimental.pallas import tpu as pltpu
from jax.sharding import PartitionSpec as P

D = 2048
KWIDTH = 31
LENGTH = 128
SEQS = 3
EPS = 1e-06
F32 = jnp.float32
BF16 = jnp.bfloat16

EIGHT = ((0, 1), (7, 8), (1, 2), (6, 7), (2, 3), (5, 6), (3, 4), (4, 5))
FOUR = ((0, 1), (6, 8), (1, 3), (3, 6))


class Way:
    def __init__(self, rows, cut, groups, relay, y, c, far, direct, cuts, bias):
        self.low, self.high = rows
        self.cut, self.groups, self.relay = cut, groups, relay
        self.y, self.c, self.far, self.direct, self.cuts, self.bias = y, c, far, direct, cuts, bias


COLUMNS = {"vg": 512, "mx": 256, "up": 768, "dn": 768}
WAYS = {
    "vg": Way((0, 64), 32, EIGHT, "FRRFFRRF", "three", "ring", "FFFFRR", True, (0, 1, 2, 3, 4), -1.9),
    "mx": Way((0, 64), 48, FOUR, "FRRF", "ring", "ring", "FRFFRR", False, (0, 2, 4), -0.2),
    "up": Way((0, 64), 48, EIGHT, "FRRFFRRF", "ring", "ring", "RRFRRF", False, (0, 2, 4), -0.8),
    "dn": Way((0, 32), 16, FOUR, "FRRF", "three", "ring", "FRRRFR", False, (0, 4), 3.2),
    "dm": Way((32, 64), 16, FOUR, "FRFF", "ring", "ring", "RRRFRR", False, (0, 2, 4), -4.2),
}
X_GATHER = ('RRR', 'DRD')
X_SUM = ('DDD', 'DRF')

RATE = 46600.0
SIBLING_RATE = 500000.0
HOP = 3.2
FURTHER_HOP = 0.5
SIBLING_HOP = 1.0
PER_COPY = 0.08
SEND_SLACK = 3.0
WINDOW = 0.3


OPPOSITE = {"y1": "y7", "y7": "y1", "y2": "y6", "y6": "y2", "z1": "z7", "z7": "z1", "x1": "x3", "x3": "x1", "x2": "x2", "d": "d"}


class Plan:
    def __init__(self, send_sems, recv_sems):
        self.copies, self.tasks, self.bias = {}, {}, {}
        self.send_sems, self.recv_sems = send_sems, recv_sems

    def copy(self, name, src, dst, device, links, needs=(), hops=1, along=1, bias=0.0):
        size = 2 if src.dtype == BF16 else 4
        for extent in src.shape:
            size *= extent
        if links == ("d",):
            took, hop = size / SIBLING_RATE, SIBLING_HOP
        else:
            took, hop = size * along / RATE, HOP + FURTHER_HOP * (hops - 1)
        self.copies[name] = ((src, dst, *device), links, took + PER_COPY, hop, frozenset(needs))
        self.bias[name] = bias

    def task(self, name, fn, needs, time):
        self.tasks[name] = (fn, frozenset(needs), time)

    def tails(self):
        own = {n: took + hop for n, (_, _, took, hop, _) in self.copies.items()}
        own.update({n: time for n, (_, _, time) in self.tasks.items()})
        users = {n: [] for n in own}
        for table in (self.copies, self.tasks):
            for n, entry in table.items():
                for need in entry[-1] if table is self.copies else entry[1]:
                    users[need].append(n)
        tails = {}

        def tail(n):
            if n not in tails:
                tails[n] = own[n] + max((tail(u) for u in users[n]), default=0.0)
            return tails[n]

        for n in own:
            tail(n)
        return tails

    def emit(self):
        now, step, done, free = 0.0, 0, set(), {}
        tails = self.tails()
        arrives, tasks = {}, dict(self.tasks)
        order = sorted(self.copies, key=lambda n: -tails[n] - self.bias[n])
        waiting = {n: self.copies[n] for n in order}
        started, started_at, heard, sends, receives, n_sends = {}, {}, {}, [], [], 0
        while waiting or arrives or tasks:
            later = []
            for name in list(waiting):
                (src, dst, where, device), links, took, hop, needs = waiting[name]
                if not needs <= done:
                    continue
                busy = max(free.get(link, 0.0) for link in links)
                if busy - now < WINDOW:
                    for link in links:
                        free[link] = max(free.get(link, 0.0), now) + took
                    left = max(free[link] for link in links)
                    arrives[name] = left + hop
                    if sends and sends[0][0] + SEND_SLACK < now:
                        _, send, last = sends.pop(0)
                        last.wait_send()
                    else:
                        send, n_sends = n_sends, n_sends + 1
                    known = heard.get(OPPOSITE.get(where), -1)
                    receive = next((r for r, at in enumerate(receives) if at < known), len(receives))
                    receives[receive : receive + 1] = [1 << 30]
                    step += 1
                    started_at[name] = step
                    descriptor = pltpu.make_async_remote_copy(
                        src_ref=src,
                        dst_ref=dst,
                        send_sem=self.send_sems.at[send],
                        recv_sem=self.recv_sems.at[receive],
                        device_id=device,
                        device_id_type=pl.DeviceIdType.MESH,
                    )
                    descriptor.start()
                    started[name] = descriptor, where, receive
                    sends.append((left, send, descriptor))
                    sends.sort(key=lambda entry: entry[:2])
                    del waiting[name]
                else:
                    later.append(busy - WINDOW + 0.001)
            here = [n for n in arrives if arrives[n] <= now]
            if here:
                first = min(here, key=lambda n: arrives[n])
                descriptor, where, receive = started.pop(first)
                descriptor.wait_recv()
                step += 1
                receives[receive] = step
                heard[where] = max(heard.get(where, -1), started_at[first])
                del arrives[first]
                done.add(first)
                now += 0.02
                continue
            ready = [n for n in tasks if tasks[n][1] <= done]
            if ready:
                best = max(ready, key=lambda n: tails[n])
                fn, _, time = tasks.pop(best)
                fn()
                done.add(best)
                now += time
                continue
            now = max(now, min(later + list(arrives.values()))) + 1e-6
        for _, _, descriptor in sends:
            descriptor.wait_send()
        assert n_sends <= SEND_SEMS and len(receives) <= RECEIVE_SEMS, (n_sends, len(receives))
        return now


def kernel(
    states, w_value, w_gate, w_mix, w_up, w_down, conv, chan, mix_hbm, mlp_hbm, out,
    vg, mx, up, dn, full, taps, chan_own, padded, filtered, stats, stats_in, activated, hidden,
    mix_gain, mlp_gain, local_sems, send_sems, recv_sems, *buffers,
):
    rep, fs, tp = lax.axis_index("rep"), lax.axis_index("fs"), lax.axis_index("tp")
    y, z_lo = lax.rem(fs, 8), fs // 8
    z = rep * 4 + z_lo
    x, core = tp // 2, lax.rem(tp, 2)
    step8, step4 = 1 + 6 * core, 1 + 2 * core

    def y_to(hops):
        return f"y{hops}", {"fs": z_lo * 8 + lax.rem(y + hops * step8, 8)}

    def z_to(hops):
        there = lax.rem(z + hops * step8, 8)
        return f"z{hops}", {"rep": there // 4, "fs": lax.rem(there, 4) * 8 + y}

    def x_to(hops):
        return f"x{hops}", {"tp": lax.rem(x + hops * step4, 4) * 2 + core}

    y_ahead, y_back, z_ahead, z_back, z_across = y_to(1), y_to(7), z_to(1), z_to(7), z_to(2)
    x_ahead, x_across, x_back = x_to(1), x_to(2), x_to(3)
    sibling = "d", {"tp": tp + 1 - 2 * core}

    own = pl.ds(pl.multiple_of(tp * 256, 256), 256)
    loads = [
        (states, full.at[0, 0, 0]),
        (w_value, vg.at[0, 0, :, 0:256]),
        (w_gate, vg.at[0, 0, :, 256:512]),
        (w_mix, mx.at[0, 0]),
        (w_up, up.at[0, 0]),
        (w_down, dn.at[0, 0]),
        (conv.at[:, own], taps),
        (chan.at[:, own], chan_own),
        (mix_hbm, mix_gain),
        (mlp_hbm, mlp_gain),
    ]
    loads = [pltpu.make_async_copy(a, b, local_sems.at[i]) for i, (a, b) in enumerate(loads)]
    for load in loads:
        load.start()

    barrier = pltpu.get_barrier_semaphore()
    peers = [y_ahead, y_back, z_ahead, z_back]
    if any(way.y != "ring" or way.c != "ring" for way in WAYS.values()):
        peers += [y_to(2), y_to(6)]
    if any(way.direct or "D" in way.relay for way in WAYS.values()):
        peers += [z_across, z_to(6)]
    peers += [("tp", {"tp": lax.rem(tp + j, 8)}) for j in range(1, 8)]
    for _, peer in peers:
        pl.semaphore_signal(
            barrier, inc=1, device_id=peer, device_id_type=pl.DeviceIdType.MESH
        )
    for tile in range(2):
        for s in range(SEQS):
            padded[tile, s, 0:32, :] = jnp.zeros((32, 128), F32)
    for load in loads:
        load.wait()
    pl.semaphore_wait(barrier, len(peers))

    plan = Plan(send_sems, recv_sems)
    wide, narrow = buffers[:7], buffers[7:]

    def along_y(name, block, how, first, far, bias):
        steps = {"F": [(8 - d, (9 - d) % 8) for d in range(1, 4)], "R": [(d, d - 1) for d in range(1, 4)]}
        if how == "ring":
            steps[far].append((4, 5) if far == "F" else (4, 3))
        for way, (link, near, over) in {"F": ("yF", y_ahead, y_to(2)), "R": ("yR", y_back, y_to(6))}.items():
            for m, before in steps[way]:
                if how == "two" and m in (2, 6):
                    plan.copy(f"{name}{m}", block(0), block(m), over, (link,), first, 2, 2, bias)
                else:
                    needs = [f"{name}{before}"] if before else first
                    plan.copy(f"{name}{m}", block(before), block(m), near, (link,), needs, bias=bias)
            if how != "ring" and way == far:
                m = 6 if far == "F" else 2
                plan.copy(f"{name}4", block(m), block(4), over, (link,), [f"{name}{m}"], 2, 2, bias)

    complete = {}
    for name, way in WAYS.items():
        ref = {"vg": vg, "mx": mx, "up": up}.get(name, dn)
        before = set(plan.copies)
        bias = way.bias
        low = pl.ds(way.low, way.cut)
        high = pl.ds(way.low + way.cut, way.high - way.low - way.cut)
        along_y(f"{name}y", lambda m, ref=ref, low=low: ref.at[m, 0, low], way.y, [], way.far[0], bias)
        for g, (lo, hi) in enumerate(way.groups):
            block = [ref.at[pl.ds(lo, hi - lo), m, low] for m in range(4)]
            needs = [f"{name}y{m}" for m in range(lo, hi) if m]
            plan.copy(f"{name}zF{g}", block[0], block[3], z_ahead, ("zF",), needs, bias=bias)
            plan.copy(f"{name}zR{g}", block[0], block[1], z_back, ("zR",), needs, bias=bias)
            if way.relay[g] == "F":
                plan.copy(f"{name}zX{g}", block[3], block[2], z_ahead, ("zF",), [f"{name}zF{g}"], bias=bias)
            elif way.relay[g] == "R":
                plan.copy(f"{name}zX{g}", block[1], block[2], z_back, ("zR",), [f"{name}zR{g}"], bias=bias)
            else:
                plan.copy(f"{name}zX{g}", block[0], block[2], z_across, ("zF", "zR"), needs, 2, bias=bias)
        block = [ref.at[0, m, high] for m in range(4)]
        plan.copy(f"{name}b3", block[0], block[3], z_ahead, ("zF",), bias=bias)
        plan.copy(f"{name}b1", block[0], block[1], z_back, ("zR",), bias=bias)
        if way.direct:
            plan.copy(f"{name}b2", block[0], block[2], z_across, ("zF", "zR"), (), 2, bias=bias)
        elif way.far[1] == "F":
            plan.copy(f"{name}b2", block[3], block[2], z_ahead, ("zF",), [f"{name}b3"], bias=bias)
        else:
            plan.copy(f"{name}b2", block[1], block[2], z_back, ("zR",), [f"{name}b1"], bias=bias)
        for i, (lo, hi) in enumerate(zip(way.cuts, way.cuts[1:])):
            at_z = pl.ds(lo, hi - lo)
            first = [f"{name}b{m}" for m in range(lo, hi) if m]
            along_y(
                f"{name}c{i}", lambda m, ref=ref, at_z=at_z, high=high: ref.at[m, at_z, high], way.c, first, way.far[2 + i], bias
            )
        complete[name] = set(plan.copies) - before

    def shards(ref, block, lo=0, hi=64):
        at_z = lax.rem((block // 2 + 4 - z_lo) * step4, 4)
        pieces = []
        for i in range(4):
            at_y = lax.rem((lax.rem(block, 2) * 4 + i + 8 - y) * step8, 8)
            pieces.append(ref[at_y, at_z, lo:hi])
        return jnp.concatenate(pieces, axis=0)

    gathered = {}
    for p in range(2):
        for s in range(SEQS):
            rows = full.at[p]
            needs = [f"mid{s}"] if p else []
            name = f"g{p}{s}"
            mine = rows.at[0, 0, s]
            plan.copy(f"{name}3", mine, rows.at[0, 3, s], x_ahead, ("xF",), needs)
            plan.copy(f"{name}1", mine, rows.at[0, 1, s], x_back, ("xR",), needs)
            if X_GATHER[p][s] == "D":
                plan.copy(f"{name}2", mine, rows.at[0, 2, s], x_across, ("xF", "xR"), needs, 2)
            elif X_GATHER[p][s] == "F":
                plan.copy(f"{name}2", rows.at[0, 3, s], rows.at[0, 2, s], x_ahead, ("xF",), [f"{name}3"])
            else:
                plan.copy(f"{name}2", rows.at[0, 1, s], rows.at[0, 2, s], x_back, ("xR",), [f"{name}1"])
            plan.copy(f"{name}S0", mine, rows.at[1, 0, s], sibling, ("d",), needs)
            for m in (1, 2, 3):
                plan.copy(f"{name}S{m}", rows.at[0, m, s], rows.at[1, 4 - m, s], sibling, ("d",), [f"{name}{m}"])
            gathered[p, s] = [name + k for k in ("3", "1", "2", "S0", "S1", "S2", "S3")]

    def normalised(p, s, gain):
        squares = jnp.zeros((LENGTH, 256), F32)
        for side in range(2):
            for at in range(4):
                values = full[p, side, at, s].astype(F32)
                squares = squares + values * values
        scale = lax.rsqrt(jnp.sum(squares, axis=-1, keepdims=True) / D + EPS)
        blocks = []
        for k in range(8):
            side = lax.rem(core + k, 2)
            at = lax.rem((k // 2 + 4 - x) * step4, 4)
            values = full[p, side, at, s].astype(F32)
            blocks.append((values * scale * gain[0:1, 256 * k : 256 * k + 256]).astype(BF16))
        return blocks

    def product(blocks, ref):
        total = None
        for k in range(8):
            term = jnp.dot(blocks[k], shards(ref, k), preferred_element_type=F32)
            total = term if total is None else total + term
        return total

    def gate_task(s):
        both = product(normalised(0, s, mix_gain), vg)
        gated = both[:, 0:256] / (1.0 + jnp.exp(-both[:, 256:512]))
        padded[0, s, 32:160, :] = gated[:, 0:128]
        padded[1, s, 32:160, :] = gated[:, 128:256]

    def filter_task(s):
        sums, squares = 0.0, 0.0
        for tile in range(2):
            lanes = slice(128 * tile, 128 * tile + 128)
            total = jnp.zeros((LENGTH, 128), F32)
            for k in range(KWIDTH):
                total = total + taps[k : k + 1, lanes] * padded[tile, s, 2 + k : 130 + k, :]
            filtered[s, :, lanes] = total
            sums = sums + total
            squares = squares + total * total
        lane = lax.broadcasted_iota(jnp.int32, (LENGTH, 128), 1)
        table = jnp.where(
            lane == 0,
            jnp.sum(sums, axis=-1, keepdims=True),
            jnp.where(lane == 1, jnp.sum(squares, axis=-1, keepdims=True), 0.0),
        )
        stats[s] = table.T[0:8, :]

    def activate_task(s):
        total = stats[s]
        for j in range(7):
            total = total + stats_in[s, j]
        table = jnp.concatenate([total, jnp.zeros((LENGTH - 8, 128), F32)], axis=0).T
        mean = table[:, 0:1] / D
        variance = table[:, 1:2] / D - mean * mean
        scale = lax.rsqrt(variance + EPS)
        v = (filtered[s] - mean) * scale * chan_own[...]
        activated[s] = (v / (1.0 + jnp.exp(-v))).astype(BF16)

    class Sums:
        def __init__(self, name, p, s, left, ref, lo, hi, how, buffers):
            self.name, self.s, self.left, self.ref, self.lo, self.hi, self.how = name, s, left, ref, lo, hi, how
            self.to_sibling, self.from_sibling, self.kept, self.sent, self.relay_part, self.relayed, self.arrived = [
                buffer.at[p, s] for buffer in buffers
            ]
            self.width = 4 * (hi - lo)
            self.direct, self.later = {"F": (3, 1), "R": (1, 3), "D": (0, 0)}[how]

        def terms(self, which):
            rows = self.left[self.s]
            at_once = 256 // self.width
            for start in range(0, 4, at_once):
                right = []
                for m in range(start, start + at_once):
                    there = lax.rem(x + m * step4, 4)
                    right.append(shards(self.ref, there * 2 + which, self.lo, self.hi))
                right = right[0] if at_once == 1 else jnp.concatenate(right, axis=0)
                both = lax.dot_general(rows, right, (((1,), (1,)), ((), ())), preferred_element_type=F32)
                for i in range(at_once):
                    yield start + i, both[:, self.width * i : self.width * (i + 1)]

        def sibling_task(self):
            for m, term in self.terms(1 - core):
                self.to_sibling[(4 - m) % 4] = term.astype(BF16)

        def own_task(self):
            for m, term in self.terms(core):
                total = term + self.from_sibling[m].astype(F32)
                if m == 0:
                    self.kept[...] = total
                elif m == self.later:
                    self.relay_part[...] = total
                else:
                    self.sent[m - 1] = total.astype(BF16)

        def relay_task(self):
            self.sent[self.later - 1] = (self.relay_part[...] + self.relayed[...].astype(F32)).astype(BF16)

        def plan(self, needs, time):
            name = self.name
            plan.task(f"{name}sib", self.sibling_task, needs, time)
            plan.copy(f"{name}D", self.to_sibling, self.from_sibling, sibling, ("d",), [f"{name}sib"])
            plan.task(f"{name}own", self.own_task, [f"{name}D"], time)
            ends = {1: (x_ahead, ("xF",)), 2: (x_across, ("xF", "xR")), 3: (x_back, ("xR",))}
            last = []
            for m in (1, 2, 3):
                if self.later and m == 2:
                    continue
                needs = [f"{name}rel"] if m == self.later else [f"{name}own"]
                last.append(f"{name}{m}")
                plan.copy(last[-1], self.sent.at[m - 1], self.arrived.at[m - 1], *ends[m], needs, 2 if m == 2 else 1)
            if self.later:
                plan.copy(f"{name}L", self.sent.at[1], self.relayed, *ends[self.later], [f"{name}own"])
                plan.task(f"{name}rel", self.relay_task, [f"{name}L", f"{name}own"], 0.1)
            return last

        def total(self):
            total = self.kept[...]
            for m in (1, 2, 3):
                if not (self.later and m == 2):
                    total = total + self.arrived[m - 1].astype(F32)
            return total

    def middle_task(s):
        full[1, 0, 0, s] = (full[0, 0, 0, s].astype(F32) + sums[0, s][0].total()).astype(BF16)

    def out_task(s):
        parts = [part.total() for part in sums[1, s]]
        if len(parts) > 1:
            parts = [part[:, 32 * i : 32 * i + 32] for i in range(4) for part in parts]
            parts = [jnp.concatenate(parts, axis=1)]
        result = full[1, 0, 0, s].astype(F32) + parts[0]
        out[LENGTH * s : LENGTH * s + LENGTH, :] = result.astype(BF16)

    def up_task(s):
        upward = jnp.maximum(product(normalised(1, s, mlp_gain), up), 0.0)
        hidden[s] = (upward * upward).astype(BF16)

    sums = {}
    for s in range(SEQS):
        plan.task(f"gate{s}", functools.partial(gate_task, s), complete["vg"] | set(gathered[0, s]), 0.35)
        plan.task(f"filter{s}", functools.partial(filter_task, s), [f"gate{s}"], 0.35)
        names = []
        for j in range(1, 8):
            names.append(f"t{s}{j}")
            peer = f"t{j}", {"tp": lax.rem(tp + j, 8)}
            plan.copy(names[-1], stats.at[s], stats_in.at[s, j - 1], peer, ("t",), [f"filter{s}"], 2)
        plan.task(f"act{s}", functools.partial(activate_task, s), names, 0.3)
        part = Sums(f"r0{s}", 0, s, activated, mx, 0, 64, X_SUM[0][s], wide)
        sums[0, s] = [part]
        plan.task(f"mid{s}", functools.partial(middle_task, s), part.plan(complete["mx"] | {f"act{s}"}, 0.25), 0.15)
        plan.task(f"up{s}", functools.partial(up_task, s), complete["up"] | set(gathered[1, s]), 0.5)
        sums[1, s], last = [], []
        for p, name in enumerate([name for name in WAYS if name in ("dn", "dm")]):
            way = WAYS[name]
            buffers = wide if way.high - way.low == 64 else narrow
            p = 1 if buffers is wide else p
            part = Sums(f"{name}{s}", p, s, hidden, dn, way.low, way.high, X_SUM[1][s], buffers)
            sums[1, s].append(part)
            last += part.plan(complete[name] | {f"up{s}"}, 0.5 if buffers is wide else 0.3)
        plan.task(f"out{s}", functools.partial(out_task, s), last, 0.15)
    plan.emit()


SEND_SEMS, RECEIVE_SEMS = 36, 91


def sum_buffers(width):
    shapes = [((4,), BF16), ((4,), BF16), ((), F32), ((3,), BF16), ((), F32), ((), BF16), ((3,), BF16)]
    return [pltpu.VMEM((2, SEQS, *lead, LENGTH, width), dtype) for lead, dtype in shapes]


def body(states, mix_gain, w_value, w_gate, conv_kernel, chan_gain, w_mix_out, mlp_gain, w_up, w_down_t):
    anywhere = pl.BlockSpec(memory_space=pltpu.HBM)
    vmem = pl.BlockSpec(memory_space=pltpu.VMEM)
    block = (LENGTH, 256)
    return pl.pallas_call(
        kernel,
        name="layer",
        out_shape=jax.ShapeDtypeStruct((SEQS * LENGTH, 256), BF16),
        in_specs=[anywhere] * 10,
        out_specs=vmem,
        scratch_shapes=[
            *[pltpu.VMEM((8, 4, 64, COLUMNS[name]), BF16) for name in ("vg", "mx", "up", "dn")],
            pltpu.VMEM((2, 2, 4, SEQS, *block), BF16),
            pltpu.VMEM((KWIDTH, 256), F32),
            pltpu.VMEM((1, 256), F32),
            pltpu.VMEM((2, SEQS, 160, 128), F32),
            pltpu.VMEM((SEQS, *block), F32),
            pltpu.VMEM((SEQS, 8, 128), F32),
            pltpu.VMEM((SEQS, 7, 8, 128), F32),
            pltpu.VMEM((SEQS, *block), BF16),
            pltpu.VMEM((SEQS, LENGTH, 768), BF16),
            pltpu.VMEM((1, D), F32),
            pltpu.VMEM((1, D), F32),
            pltpu.SemaphoreType.DMA((10,)),
            pltpu.SemaphoreType.DMA((SEND_SEMS,)),
            pltpu.SemaphoreType.DMA((RECEIVE_SEMS,)),
            *sum_buffers(256),
            *sum_buffers(128),
        ],
        compiler_params=pltpu.CompilerParams(
            collective_id=0, has_side_effects=True, vmem_limit_bytes=67043328
        ),
    )(
        states.reshape(SEQS, *block), w_value, w_gate, w_mix_out, w_up, w_down_t, conv_kernel,
        chan_gain.reshape(1, D), mix_gain.reshape(1, D), mlp_gain.reshape(1, D),
    )


def solution(mesh):
    return jax.shard_map(
        body,
        mesh=mesh,
        in_specs=(
            P(("rep", "fs"), "tp"),
            P(),
            P("fs", "tp"),
            P("fs", "tp"),
            P(),
            P(),
            P("fs", "tp"),
            P(),
            P("fs", "tp"),
            P("fs", "tp"),
        ),
        out_specs=P(("rep", "fs"), "tp"),
        check_vma=False,
    )
```

```python
import functools

import jax
import jax.numpy as jnp
from jax import lax
from jax.experimental import pallas as pl
from jax.experimental.pallas import tpu as pltpu
from jax.sharding import PartitionSpec as P

D = 2048
KWIDTH = 31
LENGTH = 128
SEQS = 3
EPS = 1e-06
F32 = jnp.float32
BF16 = jnp.bfloat16

EIGHT = ((0, 1), (7, 8), (1, 2), (6, 7), (2, 3), (5, 6), (3, 4), (4, 5))
FOUR = ((0, 1), (6, 8), (1, 3), (3, 6))


class Way:
    def __init__(self, rows, cut, groups, relay, y, c, far, direct, cuts, bias):
        self.low, self.high = rows
        self.cut, self.groups, self.relay = cut, groups, relay
        self.y, self.c, self.far, self.direct, self.cuts, self.bias = y, c, far, direct, cuts, bias


COLUMNS = {"vg": 512, "mx": 256, "up": 768, "dn": 768}
WAYS = {
    "vg": Way((0, 64), 32, EIGHT, "FRRFFRRF", "three", "ring", "FFFFRR", True, (0, 1, 2, 3, 4), -1.9),
    "mx": Way((0, 64), 48, FOUR, "FRRF", "ring", "ring", "FRFFRR", False, (0, 2, 4), -0.2),
    "up": Way((0, 64), 48, EIGHT, "FRRFFRRF", "ring", "ring", "RRFRRF", False, (0, 2, 4), -0.8),
    "dn": Way((0, 32), 16, FOUR, "FRRF", "three", "ring", "FRRRFR", False, (0, 4), 3.2),
    "dm": Way((32, 64), 16, FOUR, "FRFF", "ring", "ring", "RRRFRR", False, (0, 2, 4), -4.2),
}
X_GATHER = ('RRR', 'DRD')
X_SUM = ('DDD', 'DRF')

RATE = 46600.0
SIBLING_RATE = 500000.0
HOP = 3.35
FURTHER_HOP = 0.5
SIBLING_HOP = 1.0
PER_COPY = 0.08
SEND_SLACK = 3.0
WINDOW = 0.3


OPPOSITE = {"y1": "y7", "y7": "y1", "y2": "y6", "y6": "y2", "z1": "z7", "z7": "z1", "x1": "x3", "x3": "x1", "x2": "x2", "d": "d"}


class Plan:
    def __init__(self, send_sems, recv_sems):
        self.copies, self.tasks, self.bias = {}, {}, {}
        self.send_sems, self.recv_sems = send_sems, recv_sems

    def copy(self, name, src, dst, device, links, needs=(), hops=1, along=1, bias=0.0):
        size = 2 if src.dtype == BF16 else 4
        for extent in src.shape:
            size *= extent
        if links == ("d",):
            took, hop = size / SIBLING_RATE, SIBLING_HOP
        else:
            took, hop = size * along / RATE, HOP + FURTHER_HOP * (hops - 1)
        self.copies[name] = ((src, dst, *device), links, took + PER_COPY, hop, frozenset(needs))
        self.bias[name] = bias

    def task(self, name, fn, needs, time):
        self.tasks[name] = (fn, frozenset(needs), time)

    def tails(self):
        own = {n: took + hop for n, (_, _, took, hop, _) in self.copies.items()}
        own.update({n: time for n, (_, _, time) in self.tasks.items()})
        users = {n: [] for n in own}
        for table in (self.copies, self.tasks):
            for n, entry in table.items():
                for need in entry[-1] if table is self.copies else entry[1]:
                    users[need].append(n)
        tails = {}

        def tail(n):
            if n not in tails:
                tails[n] = own[n] + max((tail(u) for u in users[n]), default=0.0)
            return tails[n]

        for n in own:
            tail(n)
        return tails

    def emit(self):
        now, step, done, free = 0.0, 0, set(), {}
        tails = self.tails()
        arrives, tasks = {}, dict(self.tasks)
        order = sorted(self.copies, key=lambda n: -tails[n] - self.bias[n])
        waiting = {n: self.copies[n] for n in order}
        started, started_at, heard, sends, receives, n_sends = {}, {}, {}, [], [], 0
        while waiting or arrives or tasks:
            later = []
            for name in list(waiting):
                (src, dst, where, device), links, took, hop, needs = waiting[name]
                if not needs <= done:
                    continue
                busy = max(free.get(link, 0.0) for link in links)
                if busy - now < WINDOW:
                    for link in links:
                        free[link] = max(free.get(link, 0.0), now) + took
                    left = max(free[link] for link in links)
                    arrives[name] = left + hop
                    if sends and sends[0][0] + SEND_SLACK < now:
                        _, send, last = sends.pop(0)
                        last.wait_send()
                    else:
                        send, n_sends = n_sends, n_sends + 1
                    known = heard.get(OPPOSITE.get(where), -1)
                    receive = next((r for r, at in enumerate(receives) if at < known), len(receives))
                    receives[receive : receive + 1] = [1 << 30]
                    step += 1
                    started_at[name] = step
                    descriptor = pltpu.make_async_remote_copy(
                        src_ref=src,
                        dst_ref=dst,
                        send_sem=self.send_sems.at[send],
                        recv_sem=self.recv_sems.at[receive],
                        device_id=device,
                        device_id_type=pl.DeviceIdType.MESH,
                    )
                    descriptor.start()
                    started[name] = descriptor, where, receive
                    sends.append((left, send, descriptor))
                    sends.sort(key=lambda entry: entry[:2])
                    del waiting[name]
                else:
                    later.append(busy - WINDOW + 0.001)
            here = [n for n in arrives if arrives[n] <= now]
            if here:
                first = min(here, key=lambda n: arrives[n])
                descriptor, where, receive = started.pop(first)
                descriptor.wait_recv()
                step += 1
                receives[receive] = step
                heard[where] = max(heard.get(where, -1), started_at[first])
                del arrives[first]
                done.add(first)
                now += 0.02
                continue
            ready = [n for n in tasks if tasks[n][1] <= done]
            if ready:
                best = max(ready, key=lambda n: tails[n])
                fn, _, time = tasks.pop(best)
                fn()
                done.add(best)
                now += time
                continue
            now = max(now, min(later + list(arrives.values()))) + 1e-6
        for _, _, descriptor in sends:
            descriptor.wait_send()
        assert n_sends <= SEND_SEMS and len(receives) <= RECEIVE_SEMS, (n_sends, len(receives))
        return now


def kernel(
    states, w_value, w_gate, w_mix, w_up, w_down, conv, chan, mix_hbm, mlp_hbm, out,
    vg, mx, up, dn, full, taps, chan_own, padded, filtered, stats, stats_in, activated, hidden,
    mix_gain, mlp_gain, local_sems, send_sems, recv_sems, *buffers,
):
    rep, fs, tp = lax.axis_index("rep"), lax.axis_index("fs"), lax.axis_index("tp")
    y, z_lo = lax.rem(fs, 8), fs // 8
    z = rep * 4 + z_lo
    x, core = tp // 2, lax.rem(tp, 2)
    step8, step4 = 1 + 6 * core, 1 + 2 * core

    def y_to(hops):
        return f"y{hops}", {"fs": z_lo * 8 + lax.rem(y + hops * step8, 8)}

    def z_to(hops):
        there = lax.rem(z + hops * step8, 8)
        return f"z{hops}", {"rep": there // 4, "fs": lax.rem(there, 4) * 8 + y}

    def x_to(hops):
        return f"x{hops}", {"tp": lax.rem(x + hops * step4, 4) * 2 + core}

    y_ahead, y_back, z_ahead, z_back, z_across = y_to(1), y_to(7), z_to(1), z_to(7), z_to(2)
    x_ahead, x_across, x_back = x_to(1), x_to(2), x_to(3)
    sibling = "d", {"tp": tp + 1 - 2 * core}

    own = pl.ds(pl.multiple_of(tp * 256, 256), 256)
    loads = [
        (states, full.at[0, 0, 0]),
        (w_value, vg.at[0, 0, :, 0:256]),
        (w_gate, vg.at[0, 0, :, 256:512]),
        (w_mix, mx.at[0, 0]),
        (w_up, up.at[0, 0]),
        (w_down, dn.at[0, 0]),
        (conv.at[:, own], taps),
        (chan.at[:, own], chan_own),
        (mix_hbm, mix_gain),
        (mlp_hbm, mlp_gain),
    ]
    loads = [pltpu.make_async_copy(a, b, local_sems.at[i]) for i, (a, b) in enumerate(loads)]
    for load in loads:
        load.start()

    barrier = pltpu.get_barrier_semaphore()
    peers = [y_ahead, y_back, z_ahead, z_back]
    if any(way.y != "ring" or way.c != "ring" for way in WAYS.values()):
        peers += [y_to(2), y_to(6)]
    if any(way.direct or "D" in way.relay for way in WAYS.values()):
        peers += [z_across, z_to(6)]
    peers += [("tp", {"tp": lax.rem(tp + j, 8)}) for j in range(1, 8)]
    for _, peer in peers:
        pl.semaphore_signal(
            barrier, inc=1, device_id=peer, device_id_type=pl.DeviceIdType.MESH
        )
    for tile in range(2):
        for s in range(SEQS):
            padded[tile, s, 0:32, :] = jnp.zeros((32, 128), F32)
    for load in loads:
        load.wait()
    pl.semaphore_wait(barrier, len(peers))

    plan = Plan(send_sems, recv_sems)
    wide, narrow = buffers[:7], buffers[7:]

    def along_y(name, block, how, first, far, bias):
        steps = {"F": [(8 - d, (9 - d) % 8) for d in range(1, 4)], "R": [(d, d - 1) for d in range(1, 4)]}
        if how == "ring":
            steps[far].append((4, 5) if far == "F" else (4, 3))
        for way, (link, near, over) in {"F": ("yF", y_ahead, y_to(2)), "R": ("yR", y_back, y_to(6))}.items():
            for m, before in steps[way]:
                if how == "two" and m in (2, 6):
                    plan.copy(f"{name}{m}", block(0), block(m), over, (link,), first, 2, 2, bias)
                else:
                    needs = [f"{name}{before}"] if before else first
                    plan.copy(f"{name}{m}", block(before), block(m), near, (link,), needs, bias=bias)
            if how != "ring" and way == far:
                m = 6 if far == "F" else 2
                plan.copy(f"{name}4", block(m), block(4), over, (link,), [f"{name}{m}"], 2, 2, bias)

    complete = {}
    for name, way in WAYS.items():
        ref = {"vg": vg, "mx": mx, "up": up}.get(name, dn)
        before = set(plan.copies)
        bias = way.bias
        low = pl.ds(way.low, way.cut)
        high = pl.ds(way.low + way.cut, way.high - way.low - way.cut)
        along_y(f"{name}y", lambda m, ref=ref, low=low: ref.at[m, 0, low], way.y, [], way.far[0], bias)
        for g, (lo, hi) in enumerate(way.groups):
            block = [ref.at[pl.ds(lo, hi - lo), m, low] for m in range(4)]
            needs = [f"{name}y{m}" for m in range(lo, hi) if m]
            plan.copy(f"{name}zF{g}", block[0], block[3], z_ahead, ("zF",), needs, bias=bias)
            plan.copy(f"{name}zR{g}", block[0], block[1], z_back, ("zR",), needs, bias=bias)
            if way.relay[g] == "F":
                plan.copy(f"{name}zX{g}", block[3], block[2], z_ahead, ("zF",), [f"{name}zF{g}"], bias=bias)
            elif way.relay[g] == "R":
                plan.copy(f"{name}zX{g}", block[1], block[2], z_back, ("zR",), [f"{name}zR{g}"], bias=bias)
            else:
                plan.copy(f"{name}zX{g}", block[0], block[2], z_across, ("zF", "zR"), needs, 2, bias=bias)
        block = [ref.at[0, m, high] for m in range(4)]
        plan.copy(f"{name}b3", block[0], block[3], z_ahead, ("zF",), bias=bias)
        plan.copy(f"{name}b1", block[0], block[1], z_back, ("zR",), bias=bias)
        if way.direct:
            plan.copy(f"{name}b2", block[0], block[2], z_across, ("zF", "zR"), (), 2, bias=bias)
        elif way.far[1] == "F":
            plan.copy(f"{name}b2", block[3], block[2], z_ahead, ("zF",), [f"{name}b3"], bias=bias)
        else:
            plan.copy(f"{name}b2", block[1], block[2], z_back, ("zR",), [f"{name}b1"], bias=bias)
        for i, (lo, hi) in enumerate(zip(way.cuts, way.cuts[1:])):
            at_z = pl.ds(lo, hi - lo)
            first = [f"{name}b{m}" for m in range(lo, hi) if m]
            along_y(
                f"{name}c{i}", lambda m, ref=ref, at_z=at_z, high=high: ref.at[m, at_z, high], way.c, first, way.far[2 + i], bias
            )
        complete[name] = set(plan.copies) - before

    def shards(ref, block, lo=0, hi=64):
        at_z = lax.rem((block // 2 + 4 - z_lo) * step4, 4)
        pieces = []
        for i in range(4):
            at_y = lax.rem((lax.rem(block, 2) * 4 + i + 8 - y) * step8, 8)
            pieces.append(ref[at_y, at_z, lo:hi])
        return jnp.concatenate(pieces, axis=0)

    gathered = {}
    for p in range(2):
        for s in range(SEQS):
            rows = full.at[p]
            needs = [f"mid{s}"] if p else []
            name = f"g{p}{s}"
            mine = rows.at[0, 0, s]
            plan.copy(f"{name}3", mine, rows.at[0, 3, s], x_ahead, ("xF",), needs)
            plan.copy(f"{name}1", mine, rows.at[0, 1, s], x_back, ("xR",), needs)
            if X_GATHER[p][s] == "D":
                plan.copy(f"{name}2", mine, rows.at[0, 2, s], x_across, ("xF", "xR"), needs, 2)
            elif X_GATHER[p][s] == "F":
                plan.copy(f"{name}2", rows.at[0, 3, s], rows.at[0, 2, s], x_ahead, ("xF",), [f"{name}3"])
            else:
                plan.copy(f"{name}2", rows.at[0, 1, s], rows.at[0, 2, s], x_back, ("xR",), [f"{name}1"])
            plan.copy(f"{name}S0", mine, rows.at[1, 0, s], sibling, ("d",), needs)
            for m in (1, 2, 3):
                plan.copy(f"{name}S{m}", rows.at[0, m, s], rows.at[1, 4 - m, s], sibling, ("d",), [f"{name}{m}"])
            gathered[p, s] = [name + k for k in ("3", "1", "2", "S0", "S1", "S2", "S3")]

    def normalised(p, s, gain):
        squares = jnp.zeros((LENGTH, 256), F32)
        for side in range(2):
            for at in range(4):
                values = full[p, side, at, s].astype(F32)
                squares = squares + values * values
        scale = lax.rsqrt(jnp.sum(squares, axis=-1, keepdims=True) / D + EPS)
        blocks = []
        for k in range(8):
            side = lax.rem(core + k, 2)
            at = lax.rem((k // 2 + 4 - x) * step4, 4)
            values = full[p, side, at, s].astype(F32)
            blocks.append((values * scale * gain[0:1, 256 * k : 256 * k + 256]).astype(BF16))
        return blocks

    def product(blocks, ref):
        total = None
        for k in range(8):
            term = jnp.dot(blocks[k], shards(ref, k), preferred_element_type=F32)
            total = term if total is None else total + term
        return total

    def gate_task(s):
        both = product(normalised(0, s, mix_gain), vg)
        gated = both[:, 0:256] / (1.0 + jnp.exp(-both[:, 256:512]))
        padded[0, s, 32:160, :] = gated[:, 0:128]
        padded[1, s, 32:160, :] = gated[:, 128:256]

    def filter_task(s):
        sums, squares = 0.0, 0.0
        for tile in range(2):
            lanes = slice(128 * tile, 128 * tile + 128)
            total = jnp.zeros((LENGTH, 128), F32)
            for k in range(KWIDTH):
                total = total + taps[k : k + 1, lanes] * padded[tile, s, 2 + k : 130 + k, :]
            filtered[s, :, lanes] = total
            sums = sums + total
            squares = squares + total * total
        lane = lax.broadcasted_iota(jnp.int32, (LENGTH, 128), 1)
        table = jnp.where(
            lane == 0,
            jnp.sum(sums, axis=-1, keepdims=True),
            jnp.where(lane == 1, jnp.sum(squares, axis=-1, keepdims=True), 0.0),
        )
        stats[s] = table.T[0:8, :]

    def activate_task(s):
        total = stats[s]
        for j in range(7):
            total = total + stats_in[s, j]
        table = jnp.concatenate([total, jnp.zeros((LENGTH - 8, 128), F32)], axis=0).T
        mean = table[:, 0:1] / D
        variance = table[:, 1:2] / D - mean * mean
        scale = lax.rsqrt(variance + EPS)
        v = (filtered[s] - mean) * scale * chan_own[...]
        activated[s] = (v / (1.0 + jnp.exp(-v))).astype(BF16)

    class Sums:
        def __init__(self, name, p, s, left, ref, lo, hi, how, buffers):
            self.name, self.s, self.left, self.ref, self.lo, self.hi, self.how = name, s, left, ref, lo, hi, how
            self.to_sibling, self.from_sibling, self.kept, self.sent, self.relay_part, self.relayed, self.arrived = [
                buffer.at[p, s] for buffer in buffers
            ]
            self.width = 4 * (hi - lo)
            self.direct, self.later = {"F": (3, 1), "R": (1, 3), "D": (0, 0)}[how]

        def terms(self, which):
            rows = self.left[self.s]
            at_once = 256 // self.width
            for start in range(0, 4, at_once):
                right = []
                for m in range(start, start + at_once):
                    there = lax.rem(x + m * step4, 4)
                    right.append(shards(self.ref, there * 2 + which, self.lo, self.hi))
                right = right[0] if at_once == 1 else jnp.concatenate(right, axis=0)
                both = lax.dot_general(rows, right, (((1,), (1,)), ((), ())), preferred_element_type=F32)
                for i in range(at_once):
                    yield start + i, both[:, self.width * i : self.width * (i + 1)]

        def sibling_task(self):
            for m, term in self.terms(1 - core):
                self.to_sibling[(4 - m) % 4] = term.astype(BF16)

        def own_task(self):
            for m, term in self.terms(core):
                total = term + self.from_sibling[m].astype(F32)
                if m == 0:
                    self.kept[...] = total
                elif m == self.later:
                    self.relay_part[...] = total
                else:
                    self.sent[m - 1] = total.astype(BF16)

        def relay_task(self):
            self.sent[self.later - 1] = (self.relay_part[...] + self.relayed[...].astype(F32)).astype(BF16)

        def plan(self, needs, time):
            name = self.name
            plan.task(f"{name}sib", self.sibling_task, needs, time)
            plan.copy(f"{name}D", self.to_sibling, self.from_sibling, sibling, ("d",), [f"{name}sib"])
            plan.task(f"{name}own", self.own_task, [f"{name}D"], time)
            ends = {1: (x_ahead, ("xF",)), 2: (x_across, ("xF", "xR")), 3: (x_back, ("xR",))}
            last = []
            for m in (1, 2, 3):
                if self.later and m == 2:
                    continue
                needs = [f"{name}rel"] if m == self.later else [f"{name}own"]
                last.append(f"{name}{m}")
                plan.copy(last[-1], self.sent.at[m - 1], self.arrived.at[m - 1], *ends[m], needs, 2 if m == 2 else 1)
            if self.later:
                plan.copy(f"{name}L", self.sent.at[1], self.relayed, *ends[self.later], [f"{name}own"])
                plan.task(f"{name}rel", self.relay_task, [f"{name}L", f"{name}own"], 0.1)
            return last

        def total(self):
            total = self.kept[...]
            for m in (1, 2, 3):
                if not (self.later and m == 2):
                    total = total + self.arrived[m - 1].astype(F32)
            return total

    def middle_task(s):
        full[1, 0, 0, s] = (full[0, 0, 0, s].astype(F32) + sums[0, s][0].total()).astype(BF16)

    def out_task(s):
        parts = [part.total() for part in sums[1, s]]
        if len(parts) > 1:
            parts = [part[:, 32 * i : 32 * i + 32] for i in range(4) for part in parts]
            parts = [jnp.concatenate(parts, axis=1)]
        result = full[1, 0, 0, s].astype(F32) + parts[0]
        out[LENGTH * s : LENGTH * s + LENGTH, :] = result.astype(BF16)

    def up_task(s):
        upward = jnp.maximum(product(normalised(1, s, mlp_gain), up), 0.0)
        hidden[s] = (upward * upward).astype(BF16)

    sums = {}
    for s in range(SEQS):
        plan.task(f"gate{s}", functools.partial(gate_task, s), complete["vg"] | set(gathered[0, s]), 0.3)
        plan.task(f"filter{s}", functools.partial(filter_task, s), [f"gate{s}"], 0.33)
        names = []
        for j in range(1, 8):
            names.append(f"t{s}{j}")
            peer = f"t{j}", {"tp": lax.rem(tp + j, 8)}
            plan.copy(names[-1], stats.at[s], stats_in.at[s, j - 1], peer, ("t",), [f"filter{s}"], 2)
        plan.task(f"act{s}", functools.partial(activate_task, s), names, 0.2)
        part = Sums(f"r0{s}", 0, s, activated, mx, 0, 64, X_SUM[0][s], wide)
        sums[0, s] = [part]
        plan.task(f"mid{s}", functools.partial(middle_task, s), part.plan(complete["mx"] | {f"act{s}"}, 0.15), 0.15)
        plan.task(f"up{s}", functools.partial(up_task, s), complete["up"] | set(gathered[1, s]), 0.45)
        sums[1, s], last = [], []
        for p, name in enumerate([name for name in WAYS if name in ("dn", "dm")]):
            way = WAYS[name]
            buffers = wide if way.high - way.low == 64 else narrow
            p = 1 if buffers is wide else p
            part = Sums(f"{name}{s}", p, s, hidden, dn, way.low, way.high, X_SUM[1][s], buffers)
            sums[1, s].append(part)
            last += part.plan(complete[name] | {f"up{s}"}, 0.4 if buffers is wide else 0.2)
        plan.task(f"out{s}", functools.partial(out_task, s), last, 0.15)
    plan.emit()


SEND_SEMS, RECEIVE_SEMS = 36, 92


def sum_buffers(width):
    shapes = [((4,), BF16), ((4,), BF16), ((), F32), ((3,), BF16), ((), F32), ((), BF16), ((3,), BF16)]
    return [pltpu.VMEM((2, SEQS, *lead, LENGTH, width), dtype) for lead, dtype in shapes]


def body(states, mix_gain, w_value, w_gate, conv_kernel, chan_gain, w_mix_out, mlp_gain, w_up, w_down_t):
    anywhere = pl.BlockSpec(memory_space=pltpu.HBM)
    vmem = pl.BlockSpec(memory_space=pltpu.VMEM)
    block = (LENGTH, 256)
    return pl.pallas_call(
        kernel,
        name="layer",
        out_shape=jax.ShapeDtypeStruct((SEQS * LENGTH, 256), BF16),
        in_specs=[anywhere] * 10,
        out_specs=vmem,
        scratch_shapes=[
            *[pltpu.VMEM((8, 4, 64, COLUMNS[name]), BF16) for name in ("vg", "mx", "up", "dn")],
            pltpu.VMEM((2, 2, 4, SEQS, *block), BF16),
            pltpu.VMEM((KWIDTH, 256), F32),
            pltpu.VMEM((1, 256), F32),
            pltpu.VMEM((2, SEQS, 160, 128), F32),
            pltpu.VMEM((SEQS, *block), F32),
            pltpu.VMEM((SEQS, 8, 128), F32),
            pltpu.VMEM((SEQS, 7, 8, 128), F32),
            pltpu.VMEM((SEQS, *block), BF16),
            pltpu.VMEM((SEQS, LENGTH, 768), BF16),
            pltpu.VMEM((1, D), F32),
            pltpu.VMEM((1, D), F32),
            pltpu.SemaphoreType.DMA((10,)),
            pltpu.SemaphoreType.DMA((SEND_SEMS,)),
            pltpu.SemaphoreType.DMA((RECEIVE_SEMS,)),
            *sum_buffers(256),
            *sum_buffers(128),
        ],
        compiler_params=pltpu.CompilerParams(
            collective_id=0, has_side_effects=True, vmem_limit_bytes=67043328
        ),
    )(
        states.reshape(SEQS, *block), w_value, w_gate, w_mix_out, w_up, w_down_t, conv_kernel,
        chan_gain.reshape(1, D), mix_gain.reshape(1, D), mlp_gain.reshape(1, D),
    )


def solution(mesh):
    return jax.shard_map(
        body,
        mesh=mesh,
        in_specs=(
            P(("rep", "fs"), "tp"),
            P(),
            P("fs", "tp"),
            P("fs", "tp"),
            P(),
            P(),
            P("fs", "tp"),
            P(),
            P("fs", "tp"),
            P("fs", "tp"),
        ),
        out_specs=P(("rep", "fs"), "tp"),
        check_vma=False,
    )
```
